32 devices in a mesh: fs: 8 (over z, y), tp: 4 (over x, core).
Axes of the slice: x: 2, y: 2, z: 4, core: 2. Of those that a mesh axis runs over, the one named last changes fastest.
Arguments:
- tokens: bfloat16 [8192, 2048], P('fs', 'tp'), may hold values from -6 to 6
- mixer_gain: float32 [2048], replicated, may hold values from 0.1 to 1.9
- conv_taps: bfloat16 [3, 1024], replicated, may hold values from -3.5 to 3.5
- outer_weight: bfloat16 [2048, 1024], P('fs', 'tp'), may hold values from -0.125 to 0.125
- inner_weight: bfloat16 [2048, 1024], P('fs', 'tp'), may hold values from -0.125 to 0.125
- value_weight: bfloat16 [2048, 1024], P('fs', 'tp'), may hold values from -0.125 to 0.125
- merge_weight: bfloat16 [1024, 2048], P('tp', 'fs'), may hold values from -0.25 to 0.25
- merge_gain: float32 [2048], replicated, may hold values from 0.1 to 1.9
- channel_gain: float32 [2048], replicated, may hold values from 0.1 to 1.9
- gate_weight: bfloat16 [2048, 5632], P('fs', 'tp'), may hold values from -0.125 to 0.125
- up_weight: bfloat16 [2048, 5632], P('fs', 'tp'), may hold values from -0.125 to 0.125
- down_weight: bfloat16 [5632, 2048], P('tp', 'fs'), may hold values from -0.109375 to 0.109375
- output_gain: float32 [2048], replicated, may hold values from 0.1 to 1.9
Outputs:
- layer_out: bfloat16 [8192, 2048], P('fs', 'tp')
The draws below stay inside these ranges and needn't reach their ends.
All inputs are finite; a program needn't handle non-finite values.
Results may differ from the reference program's by a relative error of at most 0.018.
Values may be sent and summed in bfloat16 or wider, within the bound.
A program may use at most 128 MiB of HBM per device.

```python
import jax
import jax.numpy as jnp
from jax import lax

D = 2048
HEADS = 8
HEAD_DIM = 128
TAPS = 3
FF = 5632
SEQ = 1024
CONV_WIDTH = 1024
TOKENS = 8192
N_FS = 8
N_TP = 4


def strengthened(array, key, source, target, shards_of, factor):
    def block_of(axis_at):
        return (jnp.arange(array.shape[axis_at]) // (array.shape[axis_at] // shards_of)).reshape((-1,) + (1,) * (array.ndim - 1 - axis_at))

    first = jax.random.permutation(key, shards_of)[block_of(target)]
    far = (block_of(target) + shards_of // 2) % shards_of
    return jnp.where((block_of(source) == first) | (block_of(source) == far), factor * array, array)


def block_scale(stream_key, extent, cuts, smallest, largest):
    level, own = 1.0, jax.random.fold_in(stream_key, 6)
    for position, blocks in cuts:
        heights = jnp.exp(jax.random.uniform(jax.random.fold_in(own, position), (blocks,), jnp.float32, smallest / len(cuts), largest / len(cuts)))
        level = level * jnp.repeat(heights, extent[position] // blocks).reshape([-1 if axis == position else 1 for axis in range(len(extent))])
    return level


def gaussian(stream_key, dims, scale, bound, pieces=(), held_as=jnp.bfloat16):
    entries = scale * jax.random.normal(stream_key, dims, jnp.float32)
    if pieces:
        entries = entries * block_scale(stream_key, dims, pieces, -0.22, 0.18)
    return jnp.clip(entries, -bound, bound).astype(held_as)


def heavy_noise(own_key, shape, width, bound, cuts, heavy, dtype=jnp.bfloat16):
    array = width * jax.random.normal(own_key, shape, jnp.float32)
    if cuts:
        array = array * block_scale(own_key, shape, cuts, -0.22, 0.18)
    return jnp.clip(strengthened(array, jax.random.fold_in(own_key, 3), *heavy), -bound, bound).astype(dtype)


def setup_inputs(seed: int = 0) -> dict:
    arg_keys = jax.random.split(jax.random.key(seed), 14)
    return {
        "tokens": gaussian(arg_keys[0], (TOKENS, D), 1.0, 6.0, ((0, 8), (1, 4))),
        "mixer_gain": jnp.clip(1.0 + 0.18 * jax.random.normal(arg_keys[1], (D,), jnp.float32), 0.1, 1.9),
        "conv_taps": gaussian(arg_keys[2], (TAPS, CONV_WIDTH), TAPS ** -0.5, 3.5),
        "outer_weight": gaussian(arg_keys[3], (D, CONV_WIDTH), D ** -0.5, 0.125, ((0, 8), (1, 4))),
        "inner_weight": gaussian(arg_keys[4], (D, CONV_WIDTH), D ** -0.5, 0.125, ((0, 8), (1, 4))),
        "value_weight": gaussian(arg_keys[5], (D, CONV_WIDTH), D ** -0.5, 0.125, ((0, 8), (1, 4))),
        "merge_weight": heavy_noise(arg_keys[6], (CONV_WIDTH, D), CONV_WIDTH ** -0.5, 0.25, ((0, 4), (1, 8)), (0, 1, 8, 2.0)),
        "merge_gain": jnp.clip(1.0 + 0.18 * jax.random.normal(arg_keys[7], (D,), jnp.float32), 0.1, 1.9),
        "channel_gain": jnp.clip(1.0 + 0.18 * jax.random.normal(arg_keys[8], (D,), jnp.float32), 0.1, 1.9),
        "gate_weight": gaussian(arg_keys[9], (D, FF), D ** -0.5, 0.125, ((0, 8), (1, 4))),
        "up_weight": gaussian(arg_keys[10], (D, FF), D ** -0.5, 0.125, ((0, 8), (1, 4))),
        "down_weight": heavy_noise(arg_keys[11], (FF, D), FF ** -0.5, 0.109375, ((0, 4), (1, 8)), (0, 1, 8, 2.0)),
        "output_gain": jnp.clip(1.0 + 0.18 * jax.random.normal(arg_keys[12], (D,), jnp.float32), 0.1, 1.9),
    }


EPS = 1e-06

def normalize(values):
    floats = values.astype(jnp.float32)
    return floats * lax.rsqrt(lax.optimization_barrier(jnp.mean(floats * floats, axis=-1, keepdims=True)) + EPS)

def causal_taps(signal, taps):
    length = signal.shape[0]
    padded = jnp.pad(signal, ((2, 0), (0, 0)))
    return taps[0] * padded[:length] + taps[1] * padded[1:length + 1] + taps[2] * padded[2:]

def blocked_sum(hidden, weight):
    length = hidden.shape[0]
    block_rows = hidden.shape[1] // N_TP
    left = hidden.astype(jnp.float32).reshape(length, N_TP, block_rows)
    right = weight.astype(jnp.float32).reshape(N_TP, block_rows, weight.shape[1])
    partials = jnp.einsum('sbc,bcd->bsd', left, right)
    rounded = lax.optimization_barrier(partials.astype(jnp.bfloat16)).astype(jnp.float32)
    return lax.optimization_barrier(jnp.sum(rounded, axis=0)).astype(jnp.bfloat16)

def reference(tokens, mixer_gain, conv_taps, outer_weight, inner_weight, value_weight, merge_weight, merge_gain, channel_gain, gate_weight, up_weight, down_weight, output_gain):
    taps_float = conv_taps.astype(jnp.float32)

    def one_sequence(rows):
        normed = (normalize(rows) * mixer_gain).astype(jnp.bfloat16)
        outer = jnp.dot(normed, outer_weight, preferred_element_type=jnp.float32)
        inner = jnp.dot(normed, inner_weight, preferred_element_type=jnp.float32)
        value = jnp.dot(normed, value_weight, preferred_element_type=jnp.float32)
        conv = causal_taps(inner * value, taps_float)
        gated = (outer * conv).reshape(rows.shape[0], HEADS, HEAD_DIM)
        mixed = normalize(gated).reshape(rows.shape[0], CONV_WIDTH).astype(jnp.bfloat16)
        merged = blocked_sum(mixed, merge_weight)
        first = (rows.astype(jnp.float32) + normalize(merged) * merge_gain).astype(jnp.bfloat16)
        normed2 = (normalize(first) * channel_gain).astype(jnp.bfloat16)
        gate = jnp.dot(normed2, gate_weight, preferred_element_type=jnp.float32)
        upward = jnp.dot(normed2, up_weight, preferred_element_type=jnp.float32)
        hidden = (jax.nn.silu(gate) * upward).astype(jnp.bfloat16)
        down = blocked_sum(hidden, down_weight)
        return (first.astype(jnp.float32) + normalize(down) * output_gain).astype(jnp.bfloat16)
    outputs = lax.map(one_sequence, tokens.reshape(N_FS, SEQ, D))
    return outputs.reshape(TOKENS, D)
```

```python
import jax
import jax.numpy as jnp
from jax import lax
from jax.experimental import pallas as pl
from jax.experimental.pallas import tpu as pltpu
from jax.sharding import PartitionSpec as P

HEAD_DIM = 128
EPS = 1e-06
MESH = pl.DeviceIdType.MESH
F32 = jnp.float32
BF16 = jnp.bfloat16
MIX = (0, 1, 2, 3)
GATE, UP, DOWN = 0, 1, 2


def plane_rows(n):
    r = 1
    while 8 * r * r <= n:
        r *= 2
    return r


def layer_kernel(
    n, nt, tokens, mixer_gain, conv_taps, outer_w, inner_w, value_w, merge_w, merge_gain,
    channel_gain, gate_w, up_w, down_w, output_gain,
    out,
    toks, nrm, full_outer, full_inner, full_value, full_merge, full_gate, full_up, full_down,
    outer_s, sig, mixed, part, pa, pc, msum, first, fst, hidden, xr, zr, fr, sq_own, sq_in,
    ring_send, ring_recv, tok_send, tok_recv, pa_send, pa_recv, pc_send, pc_recv,
    z_send, z_recv, y_send, y_recv, d_send, d_recv,
    a_send, a_recv, rl_send, xr_send, xr_recv, zr_send, zr_recv, fr_send, fr_recv,
    sq_send, sq_recv,
):
    f, t = lax.axis_index("fs"), lax.axis_index("tp")
    half = n // 2
    odd = lax.rem(f, 2)
    pos = (1 - odd) * (f // 2) + odd * (n - 1 - f // 2)
    length, width = tokens.shape
    blk, channels = outer_w.shape
    cols = merge_w.shape[1]
    units = gate_w.shape[1]
    bps = n // nt
    depth = width * nt
    tile = min(256, length)
    tiles = length // tile

    yy = plane_rows(n)
    zz = n // yy
    nx = nt // 2
    z, y = f // yy, lax.rem(f, yy)
    x, c = t // 2, lax.rem(t, 2)
    p = lax.rem(z, 2)
    mate = t + 1 - 2 * c
    zpair = z + 1 - 2 * p
    zs = z - p + c
    home = p == c
    away = p != c

    def xor(a, b):
        total, bit = 0, 1
        while bit < zz:
            total = total + lax.rem(a // bit + b // bit, 2) * bit
            bit *= 2
        return total

    def at(zi, yi):
        return zi * yy + yi

    def xat(o):
        return lax.rem(x + o, nx)

    def send(src, dst, ssem, rsem, to):
        return pltpu.make_async_remote_copy(
            src_ref=src, dst_ref=dst, send_sem=ssem, recv_sem=rsem,
            device_id=to, device_id_type=MESH,
        )

    def owner(p):
        q = lax.rem(p + 2 * n, n)
        high = q // half
        return (1 - high) * (2 * q) + high * (2 * (n - 1 - q) + 1)

    right, left = owner(pos + 1), owner(pos - 1)
    rowed = {0: (outer_w, full_outer), 1: (inner_w, full_inner), 2: (value_w, full_value)}
    piece_m = channels // 2

    def own_region(w, h):
        if w in rowed:
            return rowed[w][0].at[pl.ds(h * (blk // 2), blk // 2)]
        return merge_w.at[pl.ds(h * piece_m, piece_m)]

    def region(w, h, p):
        i = owner(p)
        if w in rowed:
            start = pl.multiple_of(i * blk + h * (blk // 2), blk // 2)
            return rowed[w][1].at[pl.ds(start, blk // 2)]
        return full_merge.at[i, pl.ds(h * piece_m, piece_m)]

    def ring_copy(w, h, d, s, first=False):
        dst = region(w, h, pos - s if d == 0 else pos + s)
        return send(
            own_region(w, h) if first else dst, dst, ring_send.at[d, h, w],
            ring_recv.at[d, h, w, s], {"fs": right if d == 0 else left},
        )

    def ring_arrive(w, h, d, s):
        got = region(w, h, pos - 1 - s if d == 0 else pos + 1 + s)
        send(got, got, ring_send.at[d, h, w], ring_recv.at[d, h, w, s],
             {"fs": right if d == 0 else left}).wait_recv()

    def pieces(ws):
        return [(w, (i + d) % 2, d) for i in (0, 1) for w in ws for d in (0, 1)]

    def ring_open(ws):
        for w, h, d in pieces(ws):
            ring_copy(w, h, d, 0, True).start()

    def pump(ws, s, last=False):
        for w, h, d in pieces(ws):
            if last and h != d:
                continue
            ring_arrive(w, h, d, s - 1)
            ring_copy(w, h, d, s - 1).wait_send()
            ring_copy(w, h, d, s).start()
        for w, h, d in pieces(ws):
            if last and h != d:
                ring_arrive(w, h, d, s - 1)
                ring_copy(w, h, d, s - 1).wait_send()

    def pumps(ws, low, high):
        lax.fori_loop(low, high, lambda s, c: (pump(ws, s), c)[1], 0)

    def ring_close(ws):
        for w in ws:
            for d in (0, 1):
                ring_arrive(w, d, d, half - 1)
                ring_copy(w, d, d, half - 1).wait_send()

    def peer(o):
        return lax.rem(t + o, nt)

    offsets = range(1, nt)
    partner = mate
    strides = range(2, nt, 2)

    def hop(src, dst, ssem, rsem, i, to):
        return send(src, dst, ssem.at[i], rsem.at[i], {"tp": to})

    def gather_open(own, held, send, recv):
        for o in strides:
            hop(own, held.at[t], send, recv, o - 1, peer(o)).start()
        hop(own, held.at[t], send, recv, 0, partner).start()

    def gather_relay(own, held, send, recv):
        for o in strides:
            slab = held.at[peer(nt - o)]
            hop(own, slab, send, recv, o - 1, peer(o)).wait()
            hop(slab, slab, send, recv, o, partner).start()

    def gather_close(own, held, send, recv):
        hop(own, held.at[partner], send, recv, 0, partner).wait()
        for o in strides:
            slab = held.at[lax.rem(partner + nt - o, nt)]
            hop(held.at[peer(nt - o)], slab, send, recv, o, partner).wait()

    tok_args = (tokens, toks, tok_send, tok_recv)

    feed_in, feed_full = (gate_w, up_w), (full_gate, full_up)
    hr, hu = blk // 2, units // 2

    def feed_own(w, h):
        if w < DOWN:
            return feed_in[w].at[pl.ds(pl.multiple_of(h * hr, hr), hr)]
        return down_w.at[pl.ds(pl.multiple_of(h * hu, hu), hu)]

    def feed_region(w, g, h):
        if w < DOWN:
            return feed_full[w].at[pl.ds(pl.multiple_of(g * blk + h * hr, hr), hr)]
        return full_down.at[g, pl.ds(pl.multiple_of(h * hu, hu), hu)]

    def z_copies(w):
        for k in range(zz // 2):
            zc = 2 * xor(z // 2, k) + c
            for h in (0, 1):
                copy = send(feed_own(w, h), feed_region(w, f, h), z_send.at[w, k, h],
                            z_recv.at[w, z], {"fs": at(zc, y), "tp": 2 * x + h})
                yield jnp.logical_or(zc != z, c != h), copy

    def y_copies(w, zi, src):
        g = at(zi, y)
        for o in range(1, yy):
            yield send(src, feed_region(w, g, c), y_send.at[w, zi, o - 1], y_recv.at[w, g],
                       {"fs": at(z, lax.rem(y + o, yy))})

    def d_copy(w, g, src):
        return send(src, feed_region(w, g, c), d_send.at[w, g], d_recv.at[w, g], {"tp": mate})

    def feed_open(ws):
        for w in ws:
            @pl.when(home)
            def _():
                for copy in y_copies(w, z, feed_own(w, c)):
                    copy.start()

            for wanted, copy in z_copies(w):
                pl.when(wanted)(copy.start)

            @pl.when(home)
            def _():
                d_copy(w, f, feed_own(w, c)).start()
                if w < DOWN:
                    feed_full[w][pl.ds(pl.multiple_of(f * blk, blk), blk), :] = feed_in[w][...]
                else:
                    full_down[f] = down_w[...]

    def z_arrive(w, zi):
        got = feed_region(w, at(zi, y), c)
        send(got, got, z_send.at[w, 0, 0], z_recv.at[w, zi], {"tp": mate}).wait_recv()
        return got

    def feed_first(w):
        @pl.when(away)
        def _():
            got = z_arrive(w, z)
            for copy in y_copies(w, z, got):
                copy.start()

    def feed_relay(w, o):
        zi = xor(z, o)
        got = z_arrive(w, zi)
        for copy in y_copies(w, zi, got):
            copy.start()
        d_copy(w, at(zi, y), got).start()

    def feed_share(w, o, j):
        g = at(xor(z, o), lax.rem(y + j, yy))
        got = feed_region(w, g, c)
        send(got, got, y_send.at[w, 0, 0], y_recv.at[w, g], {"tp": mate}).wait_recv()
        d_copy(w, g, got).start()

    def feed_shares(w):
        for j in range(1, yy):
            lax.fori_loop(0, zz, lambda o, s: (feed_share(w, o, j), s)[1], 0)

    def d_arrive(w, g):
        got = feed_region(w, g, 1 - c)
        send(got, got, d_send.at[w, g], d_recv.at[w, g], {"tp": mate}).wait_recv()

    def feed_ready(w):
        def body(g, s):
            @pl.when(jnp.logical_or(g != f, away))
            def _():
                d_arrive(w, g)
            return s

        lax.fori_loop(0, n, body, 0)

    def feed_close():
        for w in (GATE, UP, DOWN):
            for wanted, copy in z_copies(w):
                pl.when(wanted)(copy.wait_send)

            def rows_done(zi, s):
                for copy in y_copies(w, zi, feed_own(w, c)):
                    copy.wait_send()
                return s

            def pieces_done(g, s):
                @pl.when(jnp.logical_or(g != f, home))
                def _():
                    d_copy(w, g, feed_own(w, c)).wait_send()
                return s

            lax.fori_loop(0, zz, rows_done, 0)
            lax.fori_loop(0, n, pieces_done, 0)

    barrier = pltpu.get_barrier_semaphore()
    greet = [{"fs": left}, {"fs": right}] + [{"tp": peer(o)} for o in offsets]
    greet += [{"fs": at(z, lax.rem(y + o, yy))} for o in range(1, yy)]
    greet += [{"fs": at(xor(z, o), y), "tp": 2 * x + h} for o in range(1, zz) for h in (0, 1)]
    for to in greet:
        pl.semaphore_signal(barrier, inc=1, device_id=to, device_id_type=MESH)
    pl.semaphore_wait(barrier, len(greet))

    ring_open(MIX)
    gather_open(*tok_args)

    own_rows = pl.ds(pl.multiple_of(f * blk, blk), blk)
    for source, full in rowed.values():
        full[own_rows, :] = source[...]
    full_merge[f] = merge_w[...]
    toks[t] = tokens[...]
    sig[pl.ds(0, 8), :] = jnp.zeros((8, channels), F32)

    pumps(MIX, 1, half - 1)
    gather_relay(*tok_args)
    pump(MIX, half - 1, True)
    feed_open((GATE, UP))
    gather_close(*tok_args)
    taps = conv_taps[:, pl.ds(pl.multiple_of(t * channels, channels), channels)].astype(F32)

    def rows_of(i):
        return pl.ds(pl.multiple_of(i * tile, tile), tile)

    def norm_tile(i, c):
        rows = rows_of(i)
        squares = jnp.zeros((tile, 1), F32)
        for j in range(nt):
            x = toks[j, rows, :].astype(F32)
            squares += jnp.sum(x * x, axis=1, keepdims=True)
        factor = lax.rsqrt(squares / depth + EPS)
        for j in range(nt):
            x = toks[j, rows, :].astype(F32)
            nrm[rows, pl.ds(j * width, width)] = (x * factor * mixer_gain[j]).astype(BF16)
        return c

    lax.fori_loop(0, tiles, norm_tile, 0)
    feed_first(GATE)
    feed_first(UP)
    ring_close(MIX)

    def project(i, c):
        rows = rows_of(i)
        x = nrm[rows, :]
        outer_s[rows, :] = jnp.dot(x, full_outer[...], preferred_element_type=F32)
        inner = jnp.dot(x, full_inner[...], preferred_element_type=F32)
        value = jnp.dot(x, full_value[...], preferred_element_type=F32)
        sig[pl.ds(pl.multiple_of(i * tile + 8, 8), tile), :] = inner * value
        return c

    lax.fori_loop(0, tiles, project, 0)
    for i in range(tiles):
        r = i * tile
        conv = (
            taps[0:1, :] * sig[r + 6 : r + 6 + tile, :]
            + taps[1:2, :] * sig[r + 7 : r + 7 + tile, :]
            + taps[2:3, :] * sig[r + 8 : r + 8 + tile, :]
        )
        gated = outer_s[r : r + tile, :] * conv
        for h in range(channels // HEAD_DIM):
            g = gated[:, h * HEAD_DIM : (h + 1) * HEAD_DIM]
            level = lax.rsqrt(jnp.mean(g * g, axis=1, keepdims=True) + EPS)
            mixed[r : r + tile, h * HEAD_DIM : (h + 1) * HEAD_DIM] = (g * level).astype(BF16)

    def merge_block(b):
        part[b] = jnp.dot(mixed[...], full_merge[b], preferred_element_type=F32).astype(BF16)

    def pair_copy(o, q):
        b = (2 * xat(o) + 1 - c) * bps + q
        return b, send(part.at[b], pa.at[o, q], pa_send.at[o, q], pa_recv.at[o, q], {"tp": mate})

    def pair_send(o, q):
        b, copy = pair_copy(o, q)
        merge_block(b)
        copy.start()

    def cross_copy(o, q):
        b = (2 * xat(o) + c) * bps + q
        return b, send(part.at[b], pc.at[o - 1, q], pc_send.at[o - 1, q], pc_recv.at[o - 1, q],
                       {"tp": 2 * xat(o) + c})

    def add_into(b, others):
        def body(i, s):
            rows = rows_of(i)
            total = part[b, rows, :].astype(F32)
            for other in others:
                total += other[rows, :].astype(F32)
            part[b, rows, :] = total.astype(BF16)
            return s

        lax.fori_loop(0, tiles, body, 0)

    each_block = [(o, q) for o in range(1, nx) for q in range(bps)]
    feed_relay(GATE, 1)
    for o, q in each_block:
        pair_send(o, q)
    for o, q in each_block:
        b, copy = cross_copy(o, q)
        merge_block(b)
        pair_copy(o, q)[1].wait_recv()
        add_into(b, [pa.at[o, q]])
        copy.start()
    for q in range(bps):
        pair_send(0, q)
    for q in range(bps):
        merge_block(t * bps + q)

    lax.fori_loop(2, zz, lambda o, s: (feed_relay(GATE, o), s)[1], 0)
    feed_relay(UP, 1)

    for q in range(bps):
        pair_copy(0, q)[1].wait_recv()
    for o, q in each_block:
        cross_copy(o, q)[1].wait_recv()

    def merged_tile(i, s):
        rows = rows_of(i)
        for q in range(bps):
            total = part[t * bps + q, rows, :].astype(F32) + pa[0, q, rows, :].astype(F32)
            for o in range(1, nx):
                total += pc[o - 1, q, rows, :].astype(F32)
            msum[rows, pl.ds(q * cols, cols)] = total.astype(BF16)
        return s

    lax.fori_loop(0, tiles, merged_tile, 0)

    def square_copy(k, o):
        return send(sq_own.at[k], sq_in.at[k, o - 1], sq_send.at[k, o - 1], sq_recv.at[k, o - 1],
                    {"tp": peer(o)})

    def square_open(k):
        def square_tile(i, c):
            rows = rows_of(i)
            x = msum[rows, :].astype(F32)
            sq_own[k, :, rows] = lax.dot_general(
                jnp.ones((8, width), F32), x * x, (((1,), (1,)), ((), ())),
                precision=lax.Precision.HIGHEST, preferred_element_type=F32,
            )
            return c

        lax.fori_loop(0, tiles, square_tile, 0)
        for o in offsets:
            square_copy(k, o).start()

    def square_close(k):
        for o in offsets:
            square_copy(k, o).wait()

    def level_of(k, rows):
        squares = sq_own[k, :, rows]
        for o in offsets:
            squares += sq_in[k, o - 1, :, rows]
        return lax.rsqrt(jnp.transpose(squares)[:, 0:1] / depth + EPS)

    square_open(0)
    for o in range(nx):
        for q in range(bps):
            pair_copy(o, q)[1].wait_send()
    for o, q in each_block:
        cross_copy(o, q)[1].wait_send()
    square_close(0)

    def slab(tt, r):
        return fst.at[tt, rows_of(r)]

    def first_copies(r):
        src = first.at[rows_of(r)]
        for o in range(1, nx):
            yield None, send(src, slab(t, r), a_send.at[o, r], a_recv.at[t, r],
                             {"tp": 2 * xat(o) + p})
        yield None, send(src, slab(t, r), a_send.at[nx, r], a_recv.at[t, r],
                         {"fs": at(zpair, y), "tp": 2 * x + p})
        yield away, send(src, slab(t, r), a_send.at[0, r], a_recv.at[t, r], {"tp": mate})

    def first_tile(r, s):
        rows = rows_of(r)
        level = level_of(0, rows)
        v = tokens[rows, :].astype(F32) + msum[rows, :].astype(F32) * level * merge_gain[t]
        first[rows, :] = v.astype(BF16)
        for wanted, copy in first_copies(r):
            if wanted is None:
                copy.start()
            else:
                pl.when(wanted)(copy.start)

        @pl.when(home)
        def _():
            fst[t, rows, :] = first[rows, :]
        return s

    lax.fori_loop(0, tiles, first_tile, 0)
    lax.fori_loop(2, zz, lambda o, s: (feed_relay(UP, o), s)[1], 0)
    feed_open((DOWN,))
    feed_first(DOWN)

    def slab_wait(tt, r):
        got = slab(tt, r)
        send(got, got, a_send.at[0, r], a_recv.at[tt, r], {"tp": mate}).wait_recv()
        return got

    def relay_copies(r, got, tt):
        for o in range(1, nx):
            yield send(got, got, rl_send.at[o - 1, r], a_recv.at[tt, r], {"tp": 2 * xat(o) + c})

    def pair_relay(r, got, tt, o):
        return send(got, got, rl_send.at[o - 1, r], a_recv.at[tt, r], {"fs": at(zpair, y)})

    def first_relay(r):
        @pl.when(home)
        def _():
            for o in range(1, nx):
                tt = 2 * xat(o) + 1
                pair_relay(r, slab_wait(tt, r), tt, o).start()

        @pl.when(away)
        def _():
            got = slab_wait(2 * x, r)
            for copy in relay_copies(r, got, 2 * x):
                copy.start()

    def first_rest(r):
        @pl.when(home)
        def _():
            slab_wait(mate, r)
            for o in range(1, nx):
                slab_wait(2 * xat(o), r)

        @pl.when(away)
        def _():
            slab_wait(2 * x + 1, r)
            for o in range(1, nx):
                slab_wait(2 * xat(o), r)
                slab_wait(2 * xat(o) + 1, r)

    def first_done(r, s):
        for wanted, copy in first_copies(r):
            if wanted is None:
                copy.wait_send()
            else:
                pl.when(wanted)(copy.wait_send)
        for copy in relay_copies(r, slab(t, r), t):
            copy.wait_send()
        return s

    def feed_norm(r):
        rows = rows_of(r)
        squares = jnp.zeros((tile, 1), F32)
        for j in range(nt):
            v = fst[j, rows, :].astype(F32)
            squares += jnp.sum(v * v, axis=1, keepdims=True)
        factor = lax.rsqrt(squares / depth + EPS)
        for j in range(nt):
            v = fst[j, rows, :].astype(F32)
            nrm[rows, pl.ds(j * width, width)] = (v * factor * channel_gain[j]).astype(BF16)

    feed_shares(GATE)
    first_relay(0)
    feed_shares(UP)

    def feed_tile(r, s):
        @pl.when(r + 1 < tiles)
        def _():
            first_relay(r + 1)

        first_rest(r)
        feed_norm(r)

        @pl.when(r == 0)
        def _():
            feed_ready(GATE)
            feed_ready(UP)

        rows = rows_of(r)
        v = nrm[rows, :]
        gate = jnp.dot(v, full_gate[...], preferred_element_type=F32)
        upward = jnp.dot(v, full_up[...], preferred_element_type=F32)
        hidden[rows, :] = (gate / (1.0 + jnp.exp(-gate)) * upward).astype(BF16)
        lax.fori_loop(
            1 + r * (zz - 1) // tiles, 1 + (r + 1) * (zz - 1) // tiles,
            lambda o, q: (feed_relay(DOWN, o), q)[1], 0,
        )
        return s

    lax.fori_loop(0, tiles, feed_tile, 0)

    def place(b):
        tt = b // bps
        return tt // 2, lax.rem(tt, 2), lax.rem(b, bps)

    def turn(xt):
        return lax.rem(x - xt + nx, nx)

    def xr_copy(b):
        xt, ct, q = place(b)
        o = turn(xt)
        return send(part.at[b], xr.at[o - 1, q], xr_send.at[b], xr_recv.at[o - 1, q],
                    {"tp": 2 * xt + c})

    def zr_copy(b):
        xt, ct, q = place(b)
        return send(part.at[b], zr.at[xt, q], zr_send.at[b], zr_recv.at[xt, q],
                    {"fs": at(zs, y)})

    def fr_copy(b, i, zt):
        xt, ct, q = place(b)
        return send(part.at[b], fr.at[q, i], fr_send.at[b], fr_recv.at[q, i],
                    {"fs": at(zt, y), "tp": 2 * xt + ct})

    def roles(b):
        xt, ct, q = place(b)
        by_x, mine = ct == 0, xt == x
        other = xt != x
        return {
            "x": (by_x & other, xr_copy(b)),
            "z": ((ct == 1) & away, zr_copy(b)),
            "collect_x": (by_x & mine, None),
            "collect_z": ((ct == 1) & home, None),
            "final_z": (by_x & mine & away, fr_copy(b, 1, zs)),
            "final_x": ((ct == 1) & home & other, fr_copy(b, turn(xt), z)),
            "final_core": (mine & home & (ct != c), fr_copy(b, 0, z)),
            "final_own": (mine & home & (ct == c), None),
        }

    def block_at(k):
        return at(xor(z, lax.rem(k, zz)), lax.rem(y + k // zz, yy))

    def down_block(k, s):
        b = block_at(k)

        @pl.when(k + 1 >= zz)
        def _():
            @pl.when(k + 1 < n)
            def _():
                feed_share(DOWN, lax.rem(k + 1, zz), (k + 1) // zz)

        @pl.when(jnp.logical_or(b != f, away))
        def _():
            d_arrive(DOWN, b)

        part[b] = jnp.dot(hidden[...], full_down[b], preferred_element_type=F32).astype(BF16)
        way = roles(b)
        for key in ("x", "z"):
            wanted, copy = way[key]
            pl.when(wanted)(copy.start)
        return s

    lax.fori_loop(0, n, down_block, 0)

    def collect(k, s):
        b = block_at(k)
        xt, ct, q = place(b)
        way = roles(b)

        @pl.when(way["collect_x"][0])
        def _():
            for o in range(1, nx):
                got = xr.at[o - 1, q]
                send(got, got, xr_send.at[b], xr_recv.at[o - 1, q], {"tp": mate}).wait_recv()
            add_into(b, [xr.at[o - 1, q] for o in range(1, nx)])

        @pl.when(way["collect_z"][0])
        def _():
            got = zr.at[xt, q]
            send(got, got, zr_send.at[b], zr_recv.at[xt, q], {"tp": mate}).wait_recv()
            add_into(b, [zr.at[xt, q]])

        for key in ("final_z", "final_x", "final_core"):
            wanted, copy = way[key]
            pl.when(wanted)(copy.start)

        @pl.when(way["final_own"][0])
        def _():
            fr[q, 0] = part[b]
        return s

    lax.fori_loop(0, n, collect, 0)

    def share_wait(q, i):
        got = fr.at[q, i]
        send(got, got, fr_send.at[0], fr_recv.at[q, i], {"tp": mate}).wait_recv()

    def final_sum(count):
        for q in range(bps):
            pl.when(away)(lambda: share_wait(q, 0))
            for i in range(1, count):
                share_wait(q, i)

            def body(i, s):
                rows = rows_of(i)
                total = fr[q, 0, rows, :].astype(F32)
                for j in range(1, count):
                    total += fr[q, j, rows, :].astype(F32)
                msum[rows, pl.ds(q * cols, cols)] = total.astype(BF16)
                return s

            lax.fori_loop(0, tiles, body, 0)

    if nx == 2:
        final_sum(2)
    else:
        pl.when(c == 0)(lambda: final_sum(2))
        pl.when(c == 1)(lambda: final_sum(nx))

    square_open(1)

    def sent(b, s):
        way = roles(b)
        for key in ("x", "z", "final_z", "final_x", "final_core"):
            wanted, copy = way[key]
            pl.when(wanted)(copy.wait_send)
        return s

    lax.fori_loop(0, n, sent, 0)
    lax.fori_loop(0, tiles, first_done, 0)
    feed_close()
    square_close(1)

    def last_tile(i, c):
        rows = rows_of(i)
        level = level_of(1, rows)
        v = first[rows, :].astype(F32) + msum[rows, :].astype(F32) * level * output_gain[t]
        out[rows, :] = v.astype(BF16)
        return c

    lax.fori_loop(0, tiles, last_tile, 0)


def solution(mesh):
    n, nt = mesh.shape["fs"], mesh.shape["tp"]

    def shards(
        tokens, mixer_gain, conv_taps, outer_weight, inner_weight, value_weight, merge_weight,
        merge_gain, channel_gain, gate_weight, up_weight, down_weight, output_gain,
    ):
        length, width = tokens.shape
        blk, channels = outer_weight.shape
        units = gate_weight.shape[1]
        cols = merge_weight.shape[1]
        depth = width * nt
        bps = n // nt
        nx = nt // 2
        yy = plane_rows(n)
        zz = n // yy
        tiles = length // min(256, length)
        most = max(2, nx)

        def slabs(gain):
            return gain.reshape(nt, 1, width)

        vmem = pl.BlockSpec(memory_space=pltpu.VMEM)
        dma = pltpu.SemaphoreType.DMA
        return pl.pallas_call(
            lambda *refs: layer_kernel(n, nt, *refs),
            out_shape=jax.ShapeDtypeStruct((length, width), BF16),
            in_specs=[vmem] * 13,
            out_specs=vmem,
            scratch_shapes=[
                pltpu.VMEM((nt, length, width), BF16),
                pltpu.VMEM((length, depth), BF16),
                pltpu.VMEM((n * blk, channels), BF16),
                pltpu.VMEM((n * blk, channels), BF16),
                pltpu.VMEM((n * blk, channels), BF16),
                pltpu.VMEM((n, channels, cols), BF16),
                pltpu.VMEM((n * blk, units), BF16),
                pltpu.VMEM((n * blk, units), BF16),
                pltpu.VMEM((n, units, cols), BF16),
                pltpu.VMEM((length, channels), F32),
                pltpu.VMEM((length + 8, channels), F32),
                pltpu.VMEM((length, channels), BF16),
                pltpu.VMEM((n, length, cols), BF16),
                pltpu.VMEM((nx, bps, length, cols), BF16),
                pltpu.VMEM((nx - 1, bps, length, cols), BF16),
                pltpu.VMEM((length, width), BF16),
                pltpu.VMEM((length, width), BF16),
                pltpu.VMEM((nt, length, width), BF16),
                pltpu.VMEM((length, units), BF16),
                pltpu.VMEM((nx - 1, bps, length, cols), BF16),
                pltpu.VMEM((nx, bps, length, cols), BF16),
                pltpu.VMEM((bps, most, length, cols), BF16),
                pltpu.VMEM((2, 8, length), F32),
                pltpu.VMEM((2, nt - 1, 8, length), F32),
                dma((2, 2, 4)),
                dma((2, 2, 4, n // 2)),
                dma((nt - 1,)), dma((nt - 1,)),
                dma((nx, bps)), dma((nx, bps)),
                dma((nx - 1, bps)), dma((nx - 1, bps)),
                dma((3, zz // 2, 2)), dma((3, zz)),
                dma((3, zz, yy - 1)), dma((3, n)),
                dma((3, n)), dma((3, n)),
                dma((nx + 1, tiles)), dma((nt, tiles)), dma((nx - 1, tiles)),
                dma((n,)), dma((nx - 1, bps)),
                dma((n,)), dma((nx, bps)),
                dma((n,)), dma((bps, most)),
                dma((2, nt - 1)), dma((2, nt - 1)),
            ],
            compiler_params=pltpu.CompilerParams(
                collective_id=0, has_side_effects=True, vmem_limit_bytes=67043328
            ),
        )(
            tokens, slabs(mixer_gain), conv_taps, outer_weight, inner_weight, value_weight,
            merge_weight, slabs(merge_gain), slabs(channel_gain), gate_weight, up_weight,
            down_weight, slabs(output_gain),
        )

    return jax.shard_map(
        shards,
        mesh=mesh,
        in_specs=(
            P("fs", "tp"), P(), P(), P("fs", "tp"), P("fs", "tp"), P("fs", "tp"), P("tp", "fs"),
            P(), P(), P("fs", "tp"), P("fs", "tp"), P("tp", "fs"), P(),
        ),
        out_specs=P("fs", "tp"),
        check_vma=False,
    )
```

```python
import functools

import jax
import jax.numpy as jnp
from jax import lax
from jax.experimental import pallas as pl
from jax.experimental.pallas import tpu as pltpu
from jax.sharding import PartitionSpec as P

HEAD_DIM = 128
EPS = 1e-06
MESH = pl.DeviceIdType.MESH
F32 = jnp.float32
BF16 = jnp.bfloat16
MIX = (0, 1, 2, 3)
GATE, UP, DOWN = 0, 1, 2
ZSHARE = 0
XSHARE = 4
DPLAN = ((1,), (), (2, 3))


def plane_rows(n):
    r = 1
    while 8 * r * r <= n:
        r *= 2
    return r


def layer_kernel(
    n, nt, tokens, mixer_gain, conv_taps, outer_w, inner_w, value_w, merge_w, merge_gain,
    channel_gain, gate_w, up_w, down_w, output_gain,
    out,
    toks, nrm, full_outer, full_inner, full_value, full_merge, full_gate, full_up, full_down,
    outer_s, sig, mixed, part, pa, pc, msum, first, fst, hidden, xr, zr, fr, sq_own, sq_in,
    ring_send, ring_recv, tok_send, tok_recv, pa_send, pa_recv, pc_send, pc_recv,
    z_send, z_recv, y_send, y_recv, d_send, d_recv,
    a_send, a_recv, rl_send, xr_send, xr_recv, zr_send, zr_recv, fr_send, fr_recv,
    sq_send, sq_recv,
):
    f, t = lax.axis_index("fs"), lax.axis_index("tp")
    half = n // 2
    odd = lax.rem(f, 2)
    pos = (1 - odd) * (f // 2) + odd * (n - 1 - f // 2)
    length, width = tokens.shape
    blk, channels = outer_w.shape
    cols = merge_w.shape[1]
    units = gate_w.shape[1]
    bps = n // nt
    depth = width * nt
    tile = min(256, length)
    tiles = length // tile

    yy = plane_rows(n)
    zz = n // yy
    nx = nt // 2
    z, y = f // yy, lax.rem(f, yy)
    x, c = t // 2, lax.rem(t, 2)
    p = lax.rem(z, 2)
    mate = t + 1 - 2 * c
    zpair = z + 1 - 2 * p
    zs = z - p + c
    home = p == c
    away = p != c

    def xor(a, b):
        total, bit = 0, 1
        while bit < zz:
            total = total + lax.rem(a // bit + b // bit, 2) * bit
            bit *= 2
        return total

    def at(zi, yi):
        return zi * yy + yi

    def xat(o):
        return lax.rem(x + o, nx)

    def send(src, dst, ssem, rsem, to):
        return pltpu.make_async_remote_copy(
            src_ref=src, dst_ref=dst, send_sem=ssem, recv_sem=rsem,
            device_id=to, device_id_type=MESH,
        )

    def owner(p):
        q = lax.rem(p + 2 * n, n)
        high = q // half
        return (1 - high) * (2 * q) + high * (2 * (n - 1 - q) + 1)

    right, left = owner(pos + 1), owner(pos - 1)
    rowed = {0: (outer_w, full_outer), 1: (inner_w, full_inner), 2: (value_w, full_value)}
    piece_m = channels // 2

    def own_region(w, h):
        if w in rowed:
            return rowed[w][0].at[pl.ds(h * (blk // 2), blk // 2)]
        return merge_w.at[pl.ds(h * piece_m, piece_m)]

    def region(w, h, p):
        i = owner(p)
        if w in rowed:
            start = pl.multiple_of(i * blk + h * (blk // 2), blk // 2)
            return rowed[w][1].at[pl.ds(start, blk // 2)]
        return full_merge.at[i, pl.ds(h * piece_m, piece_m)]

    def ring_copy(w, h, d, s, first=False):
        dst = region(w, h, pos - s if d == 0 else pos + s)
        return send(
            own_region(w, h) if first else dst, dst, ring_send.at[d, h, w],
            ring_recv.at[d, h, w, s], {"fs": right if d == 0 else left},
        )

    def ring_arrive(w, h, d, s):
        got = region(w, h, pos - 1 - s if d == 0 else pos + 1 + s)
        send(got, got, ring_send.at[d, h, w], ring_recv.at[d, h, w, s],
             {"fs": right if d == 0 else left}).wait_recv()

    def pieces(ws):
        return [(w, (i + d) % 2, d) for i in (0, 1) for w in ws for d in (0, 1)]

    def ring_open(ws):
        for w, h, d in pieces(ws):
            ring_copy(w, h, d, 0, True).start()

    def pump(ws, s, last=False):
        for w, h, d in pieces(ws):
            if last and h != d:
                continue
            ring_arrive(w, h, d, s - 1)
            ring_copy(w, h, d, s - 1).wait_send()
            ring_copy(w, h, d, s).start()
        for w, h, d in pieces(ws):
            if last and h != d:
                ring_arrive(w, h, d, s - 1)
                ring_copy(w, h, d, s - 1).wait_send()

    def pumps(ws, low, high):
        lax.fori_loop(low, high, lambda s, c: (pump(ws, s), c)[1], 0)

    def ring_close(ws):
        for w in ws:
            for d in (0, 1):
                ring_arrive(w, d, d, half - 1)
                ring_copy(w, d, d, half - 1).wait_send()

    def peer(o):
        return lax.rem(t + o, nt)

    offsets = range(1, nt)
    partner = mate
    strides = range(2, nt, 2)

    def hop(src, dst, ssem, rsem, i, to):
        return send(src, dst, ssem.at[i], rsem.at[i], {"tp": to})

    def gather_open(own, held, send, recv):
        for o in strides:
            hop(own, held.at[t], send, recv, o - 1, peer(o)).start()
        hop(own, held.at[t], send, recv, 0, partner).start()

    def gather_relay(own, held, send, recv):
        for o in strides:
            slab = held.at[peer(nt - o)]
            hop(own, slab, send, recv, o - 1, peer(o)).wait()
            hop(slab, slab, send, recv, o, partner).start()

    def gather_close(own, held, send, recv):
        hop(own, held.at[partner], send, recv, 0, partner).wait()
        for o in strides:
            slab = held.at[lax.rem(partner + nt - o, nt)]
            hop(held.at[peer(nt - o)], slab, send, recv, o, partner).wait()

    tok_args = (tokens, toks, tok_send, tok_recv)

    feed_in, feed_full = (gate_w, up_w), (full_gate, full_up)
    hr, hu = blk // 2, units // 2

    def feed_own(w, h):
        if w < DOWN:
            return feed_in[w].at[pl.ds(pl.multiple_of(h * hr, hr), hr)]
        return down_w.at[pl.ds(pl.multiple_of(h * hu, hu), hu)]

    def feed_region(w, g, h):
        if w < DOWN:
            return feed_full[w].at[pl.ds(pl.multiple_of(g * blk + h * hr, hr), hr)]
        return full_down.at[g, pl.ds(pl.multiple_of(h * hu, hu), hu)]

    OWN, INNER, OUTER, FAR = (0,), (1,), (2,), (3,)

    def z_copies(w, kinds=(0, 1, 2, 3)):
        for k in range(zz // 2):
            pair = xor(z // 2, k)
            zc = 2 * pair + c
            up = (pair > z // 2).astype(jnp.int32)
            kind = 1 + (c == up).astype(jnp.int32)
            kind = jnp.where(p == up, kind, 3) if k else 0
            for h in (0, 1):
                copy = send(feed_own(w, h), feed_region(w, f, h), z_send.at[w, k, h],
                            z_recv.at[w, z], {"fs": at(zc, y), "tp": 2 * x + h})
                if k == 0:
                    if 0 in kinds:
                        yield jnp.logical_or(zc != z, c != h), copy
                elif len(kinds) == 4:
                    yield None, copy
                else:
                    wanted = [kind == v for v in kinds if v]
                    if wanted:
                        yield functools.reduce(jnp.logical_or, wanted), copy

    def line_at(i):
        pair = xor(z // 2, i // 2)
        up = (pair > z // 2).astype(jnp.int32)
        own = 1 - jnp.minimum(i // 2, 1)
        begin = own * p + (1 - own) * (1 - up)
        return 2 * pair + begin + lax.rem(i, 2) * (1 - 2 * begin)

    def y_copies(w, zi, src):
        g = at(zi, y)
        for o in range(1, yy):
            yield send(src, feed_region(w, g, c), y_send.at[w, zi, o - 1], y_recv.at[w, g],
                       {"fs": at(z, lax.rem(y + o, yy))})

    def d_copy(w, g, src):
        return send(src, feed_region(w, g, c), d_send.at[w, g], d_recv.at[w, g], {"tp": mate})

    def start(copies):
        for wanted, copy in copies:
            if wanted is None:
                copy.start()
            else:
                pl.when(wanted)(copy.start)

    def finish(copies):
        for wanted, copy in copies:
            if wanted is None:
                copy.wait_send()
            else:
                pl.when(wanted)(copy.wait_send)

    def feed_cross(w, kinds):
        start(z_copies(w, kinds))

    def feed_open(ws):
        for w in ws:
            @pl.when(home)
            def _():
                for copy in y_copies(w, z, feed_own(w, c)):
                    copy.start()
                d_copy(w, f, feed_own(w, c)).start()
                if w < DOWN:
                    feed_full[w][pl.ds(pl.multiple_of(f * blk, blk), blk), :] = feed_in[w][...]
                else:
                    full_down[f] = down_w[...]

    def z_arrive(w, zi):
        got = feed_region(w, at(zi, y), c)
        send(got, got, z_send.at[w, 0, 0], z_recv.at[w, zi], {"tp": mate}).wait_recv()
        return got

    def feed_first(w):
        @pl.when(away)
        def _():
            got = z_arrive(w, z)
            for copy in y_copies(w, z, got):
                copy.start()

    def feed_relay(w, o):
        zi = line_at(o)
        got = z_arrive(w, zi)
        for copy in y_copies(w, zi, got):
            copy.start()
        d_copy(w, at(zi, y), got).start()

    def feed_relays(w, low, high):
        lax.fori_loop(low, high, lambda o, s: (feed_relay(w, o), s)[1], 0)

    def feed_share(w, o, j):
        g = at(line_at(o), lax.rem(y + j, yy))
        got = feed_region(w, g, c)
        send(got, got, y_send.at[w, 0, 0], y_recv.at[w, g], {"tp": mate}).wait_recv()
        d_copy(w, g, got).start()

    def feed_shares(w):
        for j in range(1, yy):
            lax.fori_loop(0, zz, lambda o, s: (feed_share(w, o, j), s)[1], 0)

    def d_arrive(w, g):
        got = feed_region(w, g, 1 - c)
        send(got, got, d_send.at[w, g], d_recv.at[w, g], {"tp": mate}).wait_recv()

    def feed_ready(w):
        def body(g, s):
            @pl.when(jnp.logical_or(g != f, away))
            def _():
                d_arrive(w, g)
            return s

        lax.fori_loop(0, n, body, 0)

    def feed_close():
        for w in (GATE, UP, DOWN):
            finish(z_copies(w))

            def rows_done(zi, s):
                for copy in y_copies(w, zi, feed_own(w, c)):
                    copy.wait_send()
                return s

            def pieces_done(g, s):
                @pl.when(jnp.logical_or(g != f, home))
                def _():
                    d_copy(w, g, feed_own(w, c)).wait_send()
                return s

            lax.fori_loop(0, zz, rows_done, 0)
            lax.fori_loop(0, n, pieces_done, 0)

    barrier = pltpu.get_barrier_semaphore()
    greet = [{"fs": left}, {"fs": right}] + [{"tp": peer(o)} for o in offsets]
    greet += [{"fs": at(z, lax.rem(y + o, yy))} for o in range(1, yy)]
    greet += [{"fs": at(xor(z, o), y), "tp": 2 * x + h} for o in range(1, zz) for h in (0, 1)]
    for to in greet:
        pl.semaphore_signal(barrier, inc=1, device_id=to, device_id_type=MESH)
    pl.semaphore_wait(barrier, len(greet))

    ring_open(MIX)
    gather_open(*tok_args)

    own_rows = pl.ds(pl.multiple_of(f * blk, blk), blk)
    for source, full in rowed.values():
        full[own_rows, :] = source[...]
    full_merge[f] = merge_w[...]
    toks[t] = tokens[...]
    sig[pl.ds(0, 8), :] = jnp.zeros((8, channels), F32)

    pumps(MIX, 1, half - 1)
    gather_relay(*tok_args)
    pump(MIX, half - 1, True)
    feed_cross(GATE, OWN + INNER + OUTER)
    feed_cross(UP, OWN)
    feed_cross(DOWN, OWN)
    feed_open((GATE, UP))
    gather_close(*tok_args)
    taps = conv_taps[:, pl.ds(pl.multiple_of(t * channels, channels), channels)].astype(F32)

    def rows_of(i):
        return pl.ds(pl.multiple_of(i * tile, tile), tile)

    def norm_tile(i, c):
        rows = rows_of(i)
        squares = jnp.zeros((tile, 1), F32)
        for j in range(nt):
            x = toks[j, rows, :].astype(F32)
            squares += jnp.sum(x * x, axis=1, keepdims=True)
        factor = lax.rsqrt(squares / depth + EPS)
        for j in range(nt):
            x = toks[j, rows, :].astype(F32)
            nrm[rows, pl.ds(j * width, width)] = (x * factor * mixer_gain[j]).astype(BF16)
        return c

    lax.fori_loop(0, tiles, norm_tile, 0)
    feed_first(GATE)
    feed_first(UP)
    ring_close(MIX)

    def project(i, c):
        rows = rows_of(i)
        x = nrm[rows, :]
        outer_s[rows, :] = jnp.dot(x, full_outer[...], preferred_element_type=F32)
        inner = jnp.dot(x, full_inner[...], preferred_element_type=F32)
        value = jnp.dot(x, full_value[...], preferred_element_type=F32)
        sig[pl.ds(pl.multiple_of(i * tile + 8, 8), tile), :] = inner * value
        return c

    lax.fori_loop(0, tiles, project, 0)
    for i in range(tiles):
        r = i * tile
        conv = (
            taps[0:1, :] * sig[r + 6 : r + 6 + tile, :]
            + taps[1:2, :] * sig[r + 7 : r + 7 + tile, :]
            + taps[2:3, :] * sig[r + 8 : r + 8 + tile, :]
        )
        gated = outer_s[r : r + tile, :] * conv
        for h in range(channels // HEAD_DIM):
            g = gated[:, h * HEAD_DIM : (h + 1) * HEAD_DIM]
            level = lax.rsqrt(jnp.mean(g * g, axis=1, keepdims=True) + EPS)
            mixed[r : r + tile, h * HEAD_DIM : (h + 1) * HEAD_DIM] = (g * level).astype(BF16)

    def merge_block(b):
        part[b] = jnp.dot(mixed[...], full_merge[b], preferred_element_type=F32).astype(BF16)

    def pair_copy(o, q):
        b = (2 * xat(o) + 1 - c) * bps + q
        return b, send(part.at[b], pa.at[o, q], pa_send.at[o, q], pa_recv.at[o, q], {"tp": mate})

    def pair_send(o, q):
        b, copy = pair_copy(o, q)
        merge_block(b)
        copy.start()

    def cross_copy(o, q):
        b = (2 * xat(o) + c) * bps + q
        return b, send(part.at[b], pc.at[o - 1, q], pc_send.at[o - 1, q], pc_recv.at[o - 1, q],
                       {"tp": 2 * xat(o) + c})

    def add_into(b, others):
        def body(i, s):
            rows = rows_of(i)
            total = part[b, rows, :].astype(F32)
            for other in others:
                total += other[rows, :].astype(F32)
            part[b, rows, :] = total.astype(BF16)
            return s

        lax.fori_loop(0, tiles, body, 0)

    each_block = [(o, q) for o in range(1, nx) for q in range(bps)]
    for o, q in each_block:
        pair_send(o, q)
    for o, q in each_block:
        b, copy = cross_copy(o, q)
        merge_block(b)
        pair_copy(o, q)[1].wait_recv()
        add_into(b, [pa.at[o, q]])
        copy.start()
    for q in range(bps):
        pair_send(0, q)
    for q in range(bps):
        merge_block(t * bps + q)

    feed_cross(GATE, FAR)
    feed_cross(UP, INNER + OUTER + FAR)
    feed_relay(GATE, 1)
    feed_relay(UP, 1)
    feed_open((DOWN,))
    feed_first(DOWN)

    for q in range(bps):
        pair_copy(0, q)[1].wait_recv()
    for o, q in each_block:
        cross_copy(o, q)[1].wait_recv()

    def square_copy(k, o):
        return send(sq_own.at[k], sq_in.at[k, o - 1], sq_send.at[k, o - 1], sq_recv.at[k, o - 1],
                    {"tp": peer(o)})

    def squares_of(v):
        v = v.astype(F32)
        sq = v * v
        high = sq.astype(BF16)
        low = (sq - high.astype(F32)).astype(BF16)
        ones = jnp.ones((8, sq.shape[1]), BF16)
        dims = (((1,), (1,)), ((), ()))
        return (
            lax.dot_general(ones, high, dims, preferred_element_type=F32)
            + lax.dot_general(ones, low, dims, preferred_element_type=F32)
        )

    def square_open(k):
        for o in offsets:
            square_copy(k, o).start()

    def square_close(k):
        for o in offsets:
            square_copy(k, o).wait()

    def level_of(k, rows):
        squares = sq_own[k, :, rows]
        for o in offsets:
            squares += sq_in[k, o - 1, :, rows]
        return lax.rsqrt(jnp.transpose(squares)[:, 0:1] / depth + EPS)

    def merged_tile(i, s):
        rows = rows_of(i)
        squares = jnp.zeros((8, tile), F32)
        for q in range(bps):
            total = part[t * bps + q, rows, :].astype(F32) + pa[0, q, rows, :].astype(F32)
            for o in range(1, nx):
                total += pc[o - 1, q, rows, :].astype(F32)
            total = total.astype(BF16)
            msum[rows, pl.ds(q * cols, cols)] = total
            squares += squares_of(total)
        sq_own[0, :, rows] = squares
        return s

    lax.fori_loop(0, tiles, merged_tile, 0)

    square_open(0)
    for o in range(nx):
        for q in range(bps):
            pair_copy(o, q)[1].wait_send()
    for o, q in each_block:
        cross_copy(o, q)[1].wait_send()
    square_close(0)

    def slab(tt, r):
        return fst.at[tt, rows_of(r)]

    def first_copies(r):
        src = first.at[rows_of(r)]
        for o in range(1, nx):
            yield None, send(src, slab(t, r), a_send.at[o, r], a_recv.at[t, r],
                             {"tp": 2 * xat(o) + p})
        yield None, send(src, slab(t, r), a_send.at[nx, r], a_recv.at[t, r],
                         {"fs": at(zpair, y), "tp": 2 * x + p})
        yield away, send(src, slab(t, r), a_send.at[0, r], a_recv.at[t, r], {"tp": mate})

    def first_tile(r, s):
        rows = rows_of(r)
        level = level_of(0, rows)
        v = tokens[rows, :].astype(F32) + msum[rows, :].astype(F32) * level * merge_gain[t]
        first[rows, :] = v.astype(BF16)
        start(first_copies(r))

        @pl.when(home)
        def _():
            fst[t, rows, :] = first[rows, :]
        return s

    lax.fori_loop(0, tiles, first_tile, 0)
    def slab_wait(tt, r):
        got = slab(tt, r)
        send(got, got, a_send.at[0, r], a_recv.at[tt, r], {"tp": mate}).wait_recv()
        return got

    by_z = tiles * ZSHARE // 4

    def relay_copies(r, got, tt, k):
        for o in range(1, nx):
            yield send(got, got, rl_send.at[k, o - 1, r], a_recv.at[tt, r],
                       {"tp": 2 * xat(o) + c})

    def pair_relay(r, got, tt, o):
        return send(got, got, rl_send.at[1, o - 1, r], a_recv.at[tt, r], {"fs": at(zpair, y)})

    def first_relay(r):
        @pl.when(jnp.logical_and(home, r < by_z))
        def _():
            for o in range(1, nx):
                tt = 2 * xat(o) + 1
                pair_relay(r, slab_wait(tt, r), tt, o).start()

        @pl.when(away)
        def _():
            got = slab_wait(2 * x, r)
            for copy in relay_copies(r, got, 2 * x, 0):
                copy.start()

        @pl.when(jnp.logical_and(away, r >= by_z))
        def _():
            got = slab_wait(2 * x + 1, r)
            for copy in relay_copies(r, got, 2 * x + 1, 1):
                copy.start()

    def first_rest(r):
        @pl.when(home)
        def _():
            slab_wait(mate, r)
            for o in range(1, nx):
                slab_wait(2 * xat(o), r)

        @pl.when(jnp.logical_and(home, r >= by_z))
        def _():
            for o in range(1, nx):
                slab_wait(2 * xat(o) + 1, r)

        @pl.when(jnp.logical_and(away, r < by_z))
        def _():
            slab_wait(2 * x + 1, r)

        @pl.when(away)
        def _():
            for o in range(1, nx):
                slab_wait(2 * xat(o), r)
                slab_wait(2 * xat(o) + 1, r)

    def first_done(r, s):
        finish(first_copies(r))
        @pl.when(away)
        def _():
            for copy in relay_copies(r, slab(t, r), t, 0):
                copy.wait_send()

        @pl.when(away == (r >= by_z))
        def _():
            for copy in relay_copies(r, slab(t, r), t, 1):
                copy.wait_send()
        return s

    def feed_norm(r):
        rows = rows_of(r)
        squares = jnp.zeros((tile, 1), F32)
        for j in range(nt):
            v = fst[j, rows, :].astype(F32)
            squares += jnp.sum(v * v, axis=1, keepdims=True)
        factor = lax.rsqrt(squares / depth + EPS)
        for j in range(nt):
            v = fst[j, rows, :].astype(F32)
            nrm[rows, pl.ds(j * width, width)] = (v * factor * channel_gain[j]).astype(BF16)

    DFIRST, DMIDDLE, DLATER = DPLAN
    feed_relays(GATE, 2, zz)
    feed_relay(DOWN, 1)
    first_relay(0)
    feed_cross(DOWN, DFIRST)
    feed_relays(UP, 2, zz)
    first_relay(1)
    feed_cross(DOWN, DMIDDLE)
    feed_shares(GATE)
    feed_shares(UP)

    def feed_tile(r, s):
        @pl.when(r + 2 < tiles)
        def _():
            first_relay(r + 2)

        @pl.when(r == 0)
        def _():
            feed_cross(DOWN, DLATER)

        first_rest(r)
        feed_norm(r)

        @pl.when(r == 0)
        def _():
            feed_ready(GATE)
            feed_ready(UP)

        rows = rows_of(r)
        v = nrm[rows, :]
        gate = jnp.dot(v, full_gate[...], preferred_element_type=F32)
        upward = jnp.dot(v, full_up[...], preferred_element_type=F32)
        hidden[rows, :] = (gate / (1.0 + jnp.exp(-gate)) * upward).astype(BF16)
        return s

    lax.fori_loop(0, tiles, feed_tile, 0)

    def place(b):
        tt = b // bps
        return tt // 2, lax.rem(tt, 2), lax.rem(b, bps)

    def first_x(ct, q):
        return ct * bps + q < 2 * bps * XSHARE // 8

    def turn(xt):
        return lax.rem(x - xt + nx, nx)

    def xr_copy(b):
        xt, ct, q = place(b)
        o = turn(xt)
        return send(part.at[b], xr.at[o - 1, ct, q], xr_send.at[b], xr_recv.at[o - 1, ct, q],
                    {"tp": 2 * xt + c})

    def zr_copy(b):
        xt, ct, q = place(b)
        return send(part.at[b], zr.at[xt, q], zr_send.at[b], zr_recv.at[xt, q],
                    {"fs": at(zs, y)})

    def fr_copy(b, i, zt):
        xt, ct, q = place(b)
        return send(part.at[b], fr.at[q, i], fr_send.at[b], fr_recv.at[q, i],
                    {"fs": at(zt, y), "tp": 2 * xt + ct})

    def roles(b):
        xt, ct, q = place(b)
        by_x, mine = first_x(ct, q), xt == x
        by_z = jnp.logical_not(by_x)
        other = xt != x
        return {
            "x": (by_x & other, xr_copy(b)),
            "z": (by_z & away, zr_copy(b)),
            "collect_x": (by_x & mine, None),
            "collect_z": (by_z & home, None),
            "final_z": (by_x & mine & away, fr_copy(b, 1, zs)),
            "final_x": (by_z & home & other, fr_copy(b, turn(xt), z)),
            "final_core": (mine & home & (ct != c), fr_copy(b, 0, z)),
            "final_own": (mine & home & (ct == c), None),
        }

    def block_at(k):
        return at(line_at(lax.rem(k, zz)), lax.rem(y + k // zz, yy))

    def down_block(k, s):
        b = block_at(k)

        @pl.when(jnp.logical_and(k >= 1, k + 1 < zz))
        def _():
            feed_relay(DOWN, k + 1)

        @pl.when(k + 1 >= zz)
        def _():
            @pl.when(k + 1 < n)
            def _():
                feed_share(DOWN, lax.rem(k + 1, zz), (k + 1) // zz)

        @pl.when(jnp.logical_or(b != f, away))
        def _():
            d_arrive(DOWN, b)

        part[b] = jnp.dot(hidden[...], full_down[b], preferred_element_type=F32).astype(BF16)
        way = roles(b)
        for key in ("x", "z"):
            wanted, copy = way[key]
            pl.when(wanted)(copy.start)
        return s

    lax.fori_loop(0, n, down_block, 0)

    def collect(k, s):
        b = block_at(k)
        xt, ct, q = place(b)
        way = roles(b)

        @pl.when(way["collect_x"][0])
        def _():
            for o in range(1, nx):
                got = xr.at[o - 1, ct, q]
                send(got, got, xr_send.at[b], xr_recv.at[o - 1, ct, q], {"tp": mate}).wait_recv()
            add_into(b, [xr.at[o - 1, ct, q] for o in range(1, nx)])

        @pl.when(way["collect_z"][0])
        def _():
            got = zr.at[xt, q]
            send(got, got, zr_send.at[b], zr_recv.at[xt, q], {"tp": mate}).wait_recv()
            add_into(b, [zr.at[xt, q]])

        for key in ("final_z", "final_x", "final_core"):
            wanted, copy = way[key]
            pl.when(wanted)(copy.start)

        @pl.when(way["final_own"][0])
        def _():
            fr[q, 0] = part[b]
        return s

    lax.fori_loop(0, n, collect, 0)

    def share_wait(q, i):
        got = fr.at[q, i]
        send(got, got, fr_send.at[0], fr_recv.at[q, i], {"tp": mate}).wait_recv()

    def final_sum(q, count):
        pl.when(away)(lambda: share_wait(q, 0))
        for i in range(1, count):
            share_wait(q, i)

        def body(i, s):
            rows = rows_of(i)
            total = fr[q, 0, rows, :].astype(F32)
            for j in range(1, count):
                total += fr[q, j, rows, :].astype(F32)
            total = total.astype(BF16)
            msum[rows, pl.ds(q * cols, cols)] = total
            if q:
                sq_own[1, :, rows] += squares_of(total)
            else:
                sq_own[1, :, rows] = squares_of(total)
            return s

        lax.fori_loop(0, tiles, body, 0)

    for q in range(bps):
        if nx == 2:
            final_sum(q, 2)
        else:
            pl.when(first_x(c, q))(lambda: final_sum(q, 2))
            pl.when(jnp.logical_not(first_x(c, q)))(lambda: final_sum(q, nx))

    square_open(1)

    def sent(b, s):
        way = roles(b)
        for key in ("x", "z", "final_z", "final_x", "final_core"):
            wanted, copy = way[key]
            pl.when(wanted)(copy.wait_send)
        return s

    lax.fori_loop(0, n, sent, 0)
    lax.fori_loop(0, tiles, first_done, 0)
    feed_close()
    square_close(1)

    def last_tile(i, c):
        rows = rows_of(i)
        level = level_of(1, rows)
        v = first[rows, :].astype(F32) + msum[rows, :].astype(F32) * level * output_gain[t]
        out[rows, :] = v.astype(BF16)
        return c

    lax.fori_loop(0, tiles, last_tile, 0)


def solution(mesh):
    n, nt = mesh.shape["fs"], mesh.shape["tp"]

    def shards(
        tokens, mixer_gain, conv_taps, outer_weight, inner_weight, value_weight, merge_weight,
        merge_gain, channel_gain, gate_weight, up_weight, down_weight, output_gain,
    ):
        length, width = tokens.shape
        blk, channels = outer_weight.shape
        units = gate_weight.shape[1]
        cols = merge_weight.shape[1]
        depth = width * nt
        bps = n // nt
        nx = nt // 2
        yy = plane_rows(n)
        zz = n // yy
        tiles = length // min(256, length)
        most = max(2, nx)

        def slabs(gain):
            return gain.reshape(nt, 1, width)

        vmem = pl.BlockSpec(memory_space=pltpu.VMEM)
        dma = pltpu.SemaphoreType.DMA
        return pl.pallas_call(
            lambda *refs: layer_kernel(n, nt, *refs),
            out_shape=jax.ShapeDtypeStruct((length, width), BF16),
            in_specs=[vmem] * 13,
            out_specs=vmem,
            scratch_shapes=[
                pltpu.VMEM((nt, length, width), BF16),
                pltpu.VMEM((length, depth), BF16),
                pltpu.VMEM((n * blk, channels), BF16),
                pltpu.VMEM((n * blk, channels), BF16),
                pltpu.VMEM((n * blk, channels), BF16),
                pltpu.VMEM((n, channels, cols), BF16),
                pltpu.VMEM((n * blk, units), BF16),
                pltpu.VMEM((n * blk, units), BF16),
                pltpu.VMEM((n, units, cols), BF16),
                pltpu.VMEM((length, channels), F32),
                pltpu.VMEM((length + 8, channels), F32),
                pltpu.VMEM((length, channels), BF16),
                pltpu.VMEM((n, length, cols), BF16),
                pltpu.VMEM((nx, bps, length, cols), BF16),
                pltpu.VMEM((nx - 1, bps, length, cols), BF16),
                pltpu.VMEM((length, width), BF16),
                pltpu.VMEM((length, width), BF16),
                pltpu.VMEM((nt, length, width), BF16),
                pltpu.VMEM((length, units), BF16),
                pltpu.VMEM((nx - 1, 2, bps, length, cols), BF16),
                pltpu.VMEM((nx, bps, length, cols), BF16),
                pltpu.VMEM((bps, most, length, cols), BF16),
                pltpu.VMEM((2, 8, length), F32),
                pltpu.VMEM((2, nt - 1, 8, length), F32),
                dma((2, 2, 4)),
                dma((2, 2, 4, n // 2)),
                dma((nt - 1,)), dma((nt - 1,)),
                dma((nx, bps)), dma((nx, bps)),
                dma((nx - 1, bps)), dma((nx - 1, bps)),
                dma((3, zz // 2, 2)), dma((3, zz)),
                dma((3, zz, yy - 1)), dma((3, n)),
                dma((3, n)), dma((3, n)),
                dma((nx + 1, tiles)), dma((nt, tiles)), dma((2, nx - 1, tiles)),
                dma((n,)), dma((nx - 1, 2, bps)),
                dma((n,)), dma((nx, bps)),
                dma((n,)), dma((bps, most)),
                dma((2, nt - 1)), dma((2, nt - 1)),
            ],
            compiler_params=pltpu.CompilerParams(
                collective_id=0, has_side_effects=True, vmem_limit_bytes=67043328
            ),
        )(
            tokens, slabs(mixer_gain), conv_taps, outer_weight, inner_weight, value_weight,
            merge_weight, slabs(merge_gain), slabs(channel_gain), gate_weight, up_weight,
            down_weight, slabs(output_gain),
        )

    return jax.shard_map(
        shards,
        mesh=mesh,
        in_specs=(
            P("fs", "tp"), P(), P(), P("fs", "tp"), P("fs", "tp"), P("fs", "tp"), P("tp", "fs"),
            P(), P(), P("fs", "tp"), P("fs", "tp"), P("tp", "fs"), P(),
        ),
        out_specs=P("fs", "tp"),
        check_vma=False,
    )
```

```python
import functools

import jax
import jax.numpy as jnp
from jax import lax
from jax.experimental import pallas as pl
from jax.experimental.pallas import tpu as pltpu
from jax.sharding import PartitionSpec as P

HEAD_DIM = 128
EPS = 1e-06
MESH = pl.DeviceIdType.MESH
F32 = jnp.float32
BF16 = jnp.bfloat16
MIX = (0, 1, 2, 3)
GATE, UP, DOWN = 0, 1, 2
ZSHARE = 0
XSHARE = 4
DPLAN = ((1,), (), (2, 3))


def plane_rows(n):
    r = 1
    while 8 * r * r <= n:
        r *= 2
    return r


def layer_kernel(
    n, nt, tokens, mixer_gain, conv_taps, outer_w, inner_w, value_w, merge_w, merge_gain,
    channel_gain, gate_w, up_w, down_w, output_gain,
    out,
    toks, nrm, full_outer, full_inner, full_value, full_merge, full_gate, full_up, full_down,
    outer_s, sig, mixed, part, pa, pc, msum, first, fst, hidden, xr, zr, fr, sq_own, sq_in,
    ring_send, ring_recv, tok_send, tok_recv, pa_send, pa_recv, pc_send, pc_recv,
    z_send, z_recv, y_send, y_recv, d_send, d_recv,
    a_send, a_recv, rl_send, xr_send, xr_recv, zr_send, zr_recv, fr_send, fr_recv,
    sq_send, sq_recv, own_sem,
):
    f, t = lax.axis_index("fs"), lax.axis_index("tp")
    half = n // 2
    odd = lax.rem(f, 2)
    pos = (1 - odd) * (f // 2) + odd * (n - 1 - f // 2)
    length, width = tokens.shape
    blk, channels = outer_w.shape
    cols = merge_w.shape[1]
    units = gate_w.shape[1]
    bps = n // nt
    depth = width * nt
    tile = min(256, length)
    tiles = length // tile

    yy = plane_rows(n)
    zz = n // yy
    nx = nt // 2
    z, y = f // yy, lax.rem(f, yy)
    x, c = t // 2, lax.rem(t, 2)
    p = lax.rem(z, 2)
    mate = t + 1 - 2 * c
    zpair = z + 1 - 2 * p
    zs = z - p + c
    home = p == c
    away = p != c

    def xor(a, b):
        total, bit = 0, 1
        while bit < zz:
            total = total + lax.rem(a // bit + b // bit, 2) * bit
            bit *= 2
        return total

    def at(zi, yi):
        return zi * yy + yi

    def xat(o):
        return lax.rem(x + o, nx)

    def send(src, dst, ssem, rsem, to):
        return pltpu.make_async_remote_copy(
            src_ref=src, dst_ref=dst, send_sem=ssem, recv_sem=rsem,
            device_id=to, device_id_type=MESH,
        )

    def owner(p):
        q = lax.rem(p + 2 * n, n)
        high = q // half
        return (1 - high) * (2 * q) + high * (2 * (n - 1 - q) + 1)

    right, left = owner(pos + 1), owner(pos - 1)
    rowed = {0: (outer_w, full_outer), 1: (inner_w, full_inner), 2: (value_w, full_value)}
    piece_m = channels // 2

    def own_region(w, h):
        if w in rowed:
            return rowed[w][0].at[pl.ds(h * (blk // 2), blk // 2)]
        return merge_w.at[pl.ds(h * piece_m, piece_m)]

    def region(w, h, p):
        i = owner(p)
        if w in rowed:
            start = pl.multiple_of(i * blk + h * (blk // 2), blk // 2)
            return rowed[w][1].at[pl.ds(start, blk // 2)]
        return full_merge.at[i, pl.ds(h * piece_m, piece_m)]

    def ring_copy(w, h, d, s, first=False):
        dst = region(w, h, pos - s if d == 0 else pos + s)
        return send(
            own_region(w, h) if first else dst, dst, ring_send.at[d, h, w],
            ring_recv.at[d, h, w, s], {"fs": right if d == 0 else left},
        )

    def ring_arrive(w, h, d, s):
        got = region(w, h, pos - 1 - s if d == 0 else pos + 1 + s)
        send(got, got, ring_send.at[d, h, w], ring_recv.at[d, h, w, s],
             {"fs": right if d == 0 else left}).wait_recv()

    def pieces(ws):
        return [(w, (i + d) % 2, d) for i in (0, 1) for w in ws for d in (0, 1)]

    def ring_open(ws):
        for w, h, d in pieces(ws):
            ring_copy(w, h, d, 0, True).start()

    def pump(ws, s, last=False):
        for w, h, d in pieces(ws):
            if last and h != d:
                continue
            ring_arrive(w, h, d, s - 1)
            ring_copy(w, h, d, s - 1).wait_send()
            ring_copy(w, h, d, s).start()
        for w, h, d in pieces(ws):
            if last and h != d:
                ring_arrive(w, h, d, s - 1)
                ring_copy(w, h, d, s - 1).wait_send()

    def pumps(ws, low, high):
        lax.fori_loop(low, high, lambda s, c: (pump(ws, s), c)[1], 0)

    def ring_close(ws):
        for w in ws:
            for d in (0, 1):
                ring_arrive(w, d, d, half - 1)
                ring_copy(w, d, d, half - 1).wait_send()

    def peer(o):
        return lax.rem(t + o, nt)

    offsets = range(1, nt)
    partner = mate
    strides = range(2, nt, 2)

    def hop(src, dst, ssem, rsem, i, to):
        return send(src, dst, ssem.at[i], rsem.at[i], {"tp": to})

    def gather_open(own, held, send, recv):
        for o in strides:
            hop(own, held.at[t], send, recv, o - 1, peer(o)).start()
        hop(own, held.at[t], send, recv, 0, partner).start()

    def gather_relay(own, held, send, recv):
        for o in strides:
            slab = held.at[peer(nt - o)]
            hop(own, slab, send, recv, o - 1, peer(o)).wait()
            hop(slab, slab, send, recv, o, partner).start()

    def gather_close(own, held, send, recv):
        hop(own, held.at[partner], send, recv, 0, partner).wait()
        for o in strides:
            slab = held.at[lax.rem(partner + nt - o, nt)]
            hop(held.at[peer(nt - o)], slab, send, recv, o, partner).wait()

    tok_args = (tokens, toks, tok_send, tok_recv)

    feed_in, feed_full = (gate_w, up_w), (full_gate, full_up)
    hr, hu = blk // 2, units // 2

    def feed_own(w, h):
        if w < DOWN:
            return feed_in[w].at[pl.ds(pl.multiple_of(h * hr, hr), hr)]
        return down_w.at[pl.ds(pl.multiple_of(h * hu, hu), hu)]

    def feed_region(w, g, h):
        if w < DOWN:
            return feed_full[w].at[pl.ds(pl.multiple_of(g * blk + h * hr, hr), hr)]
        return full_down.at[g, pl.ds(pl.multiple_of(h * hu, hu), hu)]

    OWN, INNER, OUTER, FAR = (0,), (1,), (2,), (3,)

    def z_copies(w, kinds=(0, 1, 2, 3)):
        for k in range(zz // 2):
            pair = xor(z // 2, k)
            zc = 2 * pair + c
            up = (pair > z // 2).astype(jnp.int32)
            kind = 1 + (c == up).astype(jnp.int32)
            kind = jnp.where(p == up, kind, 3) if k else 0
            for h in (0, 1):
                copy = send(feed_own(w, h), feed_region(w, f, h), z_send.at[w, k, h],
                            z_recv.at[w, z], {"fs": at(zc, y), "tp": 2 * x + h})
                if k == 0:
                    if 0 in kinds:
                        yield jnp.logical_or(zc != z, c != h), copy
                elif len(kinds) == 4:
                    yield None, copy
                else:
                    wanted = [kind == v for v in kinds if v]
                    if wanted:
                        yield functools.reduce(jnp.logical_or, wanted), copy

    def line_at(i):
        pair = xor(z // 2, i // 2)
        up = (pair > z // 2).astype(jnp.int32)
        own = 1 - jnp.minimum(i // 2, 1)
        begin = own * p + (1 - own) * (1 - up)
        return 2 * pair + begin + lax.rem(i, 2) * (1 - 2 * begin)

    def y_copies(w, zi, src):
        g = at(zi, y)
        for o in range(1, yy):
            yield send(src, feed_region(w, g, c), y_send.at[w, zi, o - 1], y_recv.at[w, g],
                       {"fs": at(z, lax.rem(y + o, yy))})

    def d_copy(w, g, src):
        return send(src, feed_region(w, g, c), d_send.at[w, g], d_recv.at[w, g], {"tp": mate})

    def start(copies):
        for wanted, copy in copies:
            if wanted is None:
                copy.start()
            else:
                pl.when(wanted)(copy.start)

    def finish(copies):
        for wanted, copy in copies:
            if wanted is None:
                copy.wait_send()
            else:
                pl.when(wanted)(copy.wait_send)

    def feed_cross(w, kinds):
        start(z_copies(w, kinds))

    def feed_here(w):
        if w < DOWN:
            held = feed_full[w].at[pl.ds(pl.multiple_of(f * blk, blk), blk)]
            return pltpu.make_async_copy(feed_in[w], held, own_sem.at[w])
        return pltpu.make_async_copy(down_w, full_down.at[f], own_sem.at[w])

    def feed_open(ws):
        for w in ws:
            @pl.when(home)
            def _():
                for copy in y_copies(w, z, feed_own(w, c)):
                    copy.start()
                d_copy(w, f, feed_own(w, c)).start()
                feed_here(w).start()

    def z_arrive(w, zi):
        got = feed_region(w, at(zi, y), c)
        send(got, got, z_send.at[w, 0, 0], z_recv.at[w, zi], {"tp": mate}).wait_recv()
        return got

    def feed_first(w):
        @pl.when(away)
        def _():
            got = z_arrive(w, z)
            for copy in y_copies(w, z, got):
                copy.start()

    def feed_relay(w, o):
        zi = line_at(o)
        got = z_arrive(w, zi)
        for copy in y_copies(w, zi, got):
            copy.start()
        d_copy(w, at(zi, y), got).start()

    def feed_relays(w, low, high):
        lax.fori_loop(low, high, lambda o, s: (feed_relay(w, o), s)[1], 0)

    def feed_share(w, o, j):
        g = at(line_at(o), lax.rem(y + j, yy))
        got = feed_region(w, g, c)
        send(got, got, y_send.at[w, 0, 0], y_recv.at[w, g], {"tp": mate}).wait_recv()
        d_copy(w, g, got).start()

    def feed_shares(w):
        for j in range(1, yy):
            lax.fori_loop(0, zz, lambda o, s: (feed_share(w, o, j), s)[1], 0)

    def d_arrive(w, g):
        got = feed_region(w, g, 1 - c)
        send(got, got, d_send.at[w, g], d_recv.at[w, g], {"tp": mate}).wait_recv()

    def feed_ready(w):
        def body(g, s):
            @pl.when(jnp.logical_or(g != f, away))
            def _():
                d_arrive(w, g)
            return s

        lax.fori_loop(0, n, body, 0)

    def feed_close():
        for w in (GATE, UP, DOWN):
            finish(z_copies(w))

            def rows_done(zi, s):
                for copy in y_copies(w, zi, feed_own(w, c)):
                    copy.wait_send()
                return s

            def pieces_done(g, s):
                @pl.when(jnp.logical_or(g != f, home))
                def _():
                    d_copy(w, g, feed_own(w, c)).wait_send()
                return s

            lax.fori_loop(0, zz, rows_done, 0)
            lax.fori_loop(0, n, pieces_done, 0)

    barrier = pltpu.get_barrier_semaphore()
    greet = [{"fs": left}, {"fs": right}] + [{"tp": peer(o)} for o in offsets]
    greet += [{"fs": at(z, lax.rem(y + o, yy))} for o in range(1, yy)]
    greet += [{"fs": at(xor(z, o), y), "tp": 2 * x + h} for o in range(1, zz) for h in (0, 1)]
    for to in greet:
        pl.semaphore_signal(barrier, inc=1, device_id=to, device_id_type=MESH)
    pl.semaphore_wait(barrier, len(greet))

    ring_open(MIX)
    gather_open(*tok_args)

    own_rows = pl.ds(pl.multiple_of(f * blk, blk), blk)
    mix_own = [
        pltpu.make_async_copy(source, full.at[own_rows], own_sem.at[3 + w])
        for w, (source, full) in rowed.items()
    ] + [pltpu.make_async_copy(merge_w, full_merge.at[f], own_sem.at[6])]
    for copy in mix_own:
        copy.start()
    toks[t] = tokens[...]
    sig[pl.ds(0, 8), :] = jnp.zeros((8, channels), F32)

    pumps(MIX, 1, half - 1)
    gather_relay(*tok_args)
    pump(MIX, half - 1, True)
    feed_cross(GATE, OWN + INNER + OUTER)
    feed_cross(UP, OWN)
    feed_cross(DOWN, OWN)
    feed_open((GATE, UP))
    gather_close(*tok_args)
    taps = conv_taps[:, pl.ds(pl.multiple_of(t * channels, channels), channels)].astype(F32)

    def rows_of(i):
        return pl.ds(pl.multiple_of(i * tile, tile), tile)

    def norm_tile(i, c):
        rows = rows_of(i)
        squares = jnp.zeros((tile, 1), F32)
        for j in range(nt):
            x = toks[j, rows, :].astype(F32)
            squares += jnp.sum(x * x, axis=1, keepdims=True)
        factor = lax.rsqrt(squares / depth + EPS)
        for j in range(nt):
            x = toks[j, rows, :].astype(F32)
            nrm[rows, pl.ds(j * width, width)] = (x * factor * mixer_gain[j]).astype(BF16)
        return c

    lax.fori_loop(0, tiles, norm_tile, 0)
    feed_first(GATE)
    feed_first(UP)
    ring_close(MIX)
    for copy in mix_own:
        copy.wait()

    def project(i, c):
        rows = rows_of(i)
        x = nrm[rows, :]
        outer_s[rows, :] = jnp.dot(x, full_outer[...], preferred_element_type=F32)
        inner = jnp.dot(x, full_inner[...], preferred_element_type=F32)
        value = jnp.dot(x, full_value[...], preferred_element_type=F32)
        sig[pl.ds(pl.multiple_of(i * tile + 8, 8), tile), :] = inner * value
        return c

    lax.fori_loop(0, tiles, project, 0)
    for i in range(tiles):
        r = i * tile
        conv = (
            taps[0:1, :] * sig[r + 6 : r + 6 + tile, :]
            + taps[1:2, :] * sig[r + 7 : r + 7 + tile, :]
            + taps[2:3, :] * sig[r + 8 : r + 8 + tile, :]
        )
        gated = outer_s[r : r + tile, :] * conv
        for h in range(channels // HEAD_DIM):
            g = gated[:, h * HEAD_DIM : (h + 1) * HEAD_DIM]
            level = lax.rsqrt(jnp.mean(g * g, axis=1, keepdims=True) + EPS)
            mixed[r : r + tile, h * HEAD_DIM : (h + 1) * HEAD_DIM] = (g * level).astype(BF16)

    def merge_block(b):
        part[b] = jnp.dot(mixed[...], full_merge[b], preferred_element_type=F32).astype(BF16)

    def pair_copy(o, q):
        b = (2 * xat(o) + 1 - c) * bps + q
        return b, send(part.at[b], pa.at[o, q], pa_send.at[o, q], pa_recv.at[o, q], {"tp": mate})

    def pair_send(o, q):
        b, copy = pair_copy(o, q)
        merge_block(b)
        copy.start()

    def cross_copy(o, q):
        b = (2 * xat(o) + c) * bps + q
        return b, send(part.at[b], pc.at[o - 1, q], pc_send.at[o - 1, q], pc_recv.at[o - 1, q],
                       {"tp": 2 * xat(o) + c})

    def add_into(b, others):
        def body(i, s):
            rows = rows_of(i)
            total = part[b, rows, :].astype(F32)
            for other in others:
                total += other[rows, :].astype(F32)
            part[b, rows, :] = total.astype(BF16)
            return s

        lax.fori_loop(0, tiles, body, 0)

    each_block = [(o, q) for o in range(1, nx) for q in range(bps)]
    for o, q in each_block:
        pair_send(o, q)
    for o, q in each_block:
        b, copy = cross_copy(o, q)
        merge_block(b)
        pair_copy(o, q)[1].wait_recv()
        add_into(b, [pa.at[o, q]])
        copy.start()
    for q in range(bps):
        pair_send(0, q)
    for q in range(bps):
        merge_block(t * bps + q)

    feed_cross(GATE, FAR)
    feed_cross(UP, INNER + OUTER + FAR)
    feed_relay(GATE, 1)
    feed_relay(UP, 1)
    feed_open((DOWN,))
    feed_first(DOWN)

    for q in range(bps):
        pair_copy(0, q)[1].wait_recv()
    for o, q in each_block:
        cross_copy(o, q)[1].wait_recv()

    def square_copy(k, o):
        return send(sq_own.at[k], sq_in.at[k, o - 1], sq_send.at[k, o - 1], sq_recv.at[k, o - 1],
                    {"tp": peer(o)})

    def squares_of(v):
        v = v.astype(F32)
        sq = v * v
        high = sq.astype(BF16)
        low = (sq - high.astype(F32)).astype(BF16)
        ones = jnp.ones((8, sq.shape[1]), BF16)
        dims = (((1,), (1,)), ((), ()))
        return (
            lax.dot_general(ones, high, dims, preferred_element_type=F32)
            + lax.dot_general(ones, low, dims, preferred_element_type=F32)
        )

    def square_open(k):
        for o in offsets:
            square_copy(k, o).start()

    def square_close(k):
        for o in offsets:
            square_copy(k, o).wait()

    def level_of(k, rows):
        squares = sq_own[k, :, rows]
        for o in offsets:
            squares += sq_in[k, o - 1, :, rows]
        return lax.rsqrt(jnp.transpose(squares)[:, 0:1] / depth + EPS)

    def merged_tile(i, s):
        rows = rows_of(i)
        squares = jnp.zeros((8, tile), F32)
        for q in range(bps):
            total = part[t * bps + q, rows, :].astype(F32) + pa[0, q, rows, :].astype(F32)
            for o in range(1, nx):
                total += pc[o - 1, q, rows, :].astype(F32)
            total = total.astype(BF16)
            msum[rows, pl.ds(q * cols, cols)] = total
            squares += squares_of(total)
        sq_own[0, :, rows] = squares
        return s

    lax.fori_loop(0, tiles, merged_tile, 0)

    square_open(0)
    for o in range(nx):
        for q in range(bps):
            pair_copy(o, q)[1].wait_send()
    for o, q in each_block:
        cross_copy(o, q)[1].wait_send()
    square_close(0)

    def slab(tt, r):
        return fst.at[tt, rows_of(r)]

    def first_copies(r):
        src = first.at[rows_of(r)]
        for o in range(1, nx):
            yield None, send(src, slab(t, r), a_send.at[o, r], a_recv.at[t, r],
                             {"tp": 2 * xat(o) + p})
        yield None, send(src, slab(t, r), a_send.at[nx, r], a_recv.at[t, r],
                         {"fs": at(zpair, y), "tp": 2 * x + p})
        yield away, send(src, slab(t, r), a_send.at[0, r], a_recv.at[t, r], {"tp": mate})

    def first_tile(r, s):
        rows = rows_of(r)
        level = level_of(0, rows)
        v = tokens[rows, :].astype(F32) + msum[rows, :].astype(F32) * level * merge_gain[t]
        first[rows, :] = v.astype(BF16)
        start(first_copies(r))

        @pl.when(home)
        def _():
            fst[t, rows, :] = first[rows, :]
        return s

    lax.fori_loop(0, tiles, first_tile, 0)
    def slab_wait(tt, r):
        got = slab(tt, r)
        send(got, got, a_send.at[0, r], a_recv.at[tt, r], {"tp": mate}).wait_recv()
        return got

    by_z = tiles * ZSHARE // 4

    def relay_copies(r, got, tt, k):
        for o in range(1, nx):
            yield send(got, got, rl_send.at[k, o - 1, r], a_recv.at[tt, r],
                       {"tp": 2 * xat(o) + c})

    def pair_relay(r, got, tt, o):
        return send(got, got, rl_send.at[1, o - 1, r], a_recv.at[tt, r], {"fs": at(zpair, y)})

    def first_relay(r):
        @pl.when(jnp.logical_and(home, r < by_z))
        def _():
            for o in range(1, nx):
                tt = 2 * xat(o) + 1
                pair_relay(r, slab_wait(tt, r), tt, o).start()

        @pl.when(away)
        def _():
            got = slab_wait(2 * x, r)
            for copy in relay_copies(r, got, 2 * x, 0):
                copy.start()

        @pl.when(jnp.logical_and(away, r >= by_z))
        def _():
            got = slab_wait(2 * x + 1, r)
            for copy in relay_copies(r, got, 2 * x + 1, 1):
                copy.start()

    def first_rest(r):
        @pl.when(home)
        def _():
            slab_wait(mate, r)
            for o in range(1, nx):
                slab_wait(2 * xat(o), r)

        @pl.when(jnp.logical_and(home, r >= by_z))
        def _():
            for o in range(1, nx):
                slab_wait(2 * xat(o) + 1, r)

        @pl.when(jnp.logical_and(away, r < by_z))
        def _():
            slab_wait(2 * x + 1, r)

        @pl.when(away)
        def _():
            for o in range(1, nx):
                slab_wait(2 * xat(o), r)
                slab_wait(2 * xat(o) + 1, r)

    def first_done(r, s):
        finish(first_copies(r))
        @pl.when(away)
        def _():
            for copy in relay_copies(r, slab(t, r), t, 0):
                copy.wait_send()

        @pl.when(away == (r >= by_z))
        def _():
            for copy in relay_copies(r, slab(t, r), t, 1):
                copy.wait_send()
        return s

    def feed_norm(r):
        rows = rows_of(r)
        squares = jnp.zeros((tile, 1), F32)
        for j in range(nt):
            v = fst[j, rows, :].astype(F32)
            squares += jnp.sum(v * v, axis=1, keepdims=True)
        factor = lax.rsqrt(squares / depth + EPS)
        for j in range(nt):
            v = fst[j, rows, :].astype(F32)
            nrm[rows, pl.ds(j * width, width)] = (v * factor * channel_gain[j]).astype(BF16)

    DFIRST, DMIDDLE, DLATER = DPLAN
    feed_relays(GATE, 2, zz)
    feed_relay(DOWN, 1)
    first_relay(0)
    feed_cross(DOWN, DFIRST)
    feed_relays(UP, 2, zz)
    first_relay(1)
    feed_cross(DOWN, DMIDDLE)
    feed_shares(GATE)
    feed_shares(UP)

    def feed_tile(r, s):
        @pl.when(r + 2 < tiles)
        def _():
            first_relay(r + 2)

        @pl.when(r == 0)
        def _():
            feed_cross(DOWN, DLATER)

        first_rest(r)
        feed_norm(r)

        @pl.when(r == 0)
        def _():
            feed_ready(GATE)
            feed_ready(UP)

            @pl.when(home)
            def _():
                for w in (GATE, UP, DOWN):
                    feed_here(w).wait()

        rows = rows_of(r)
        v = nrm[rows, :]
        gate = jnp.dot(v, full_gate[...], preferred_element_type=F32)
        upward = jnp.dot(v, full_up[...], preferred_element_type=F32)
        hidden[rows, :] = (gate / (1.0 + jnp.exp(-gate)) * upward).astype(BF16)
        return s

    lax.fori_loop(0, tiles, feed_tile, 0)

    def place(b):
        tt = b // bps
        return tt // 2, lax.rem(tt, 2), lax.rem(b, bps)

    def first_x(ct, q):
        return ct * bps + q < 2 * bps * XSHARE // 8

    def turn(xt):
        return lax.rem(x - xt + nx, nx)

    def xr_copy(b):
        xt, ct, q = place(b)
        o = turn(xt)
        return send(part.at[b], xr.at[o - 1, ct, q], xr_send.at[b], xr_recv.at[o - 1, ct, q],
                    {"tp": 2 * xt + c})

    def zr_copy(b):
        xt, ct, q = place(b)
        return send(part.at[b], zr.at[xt, q], zr_send.at[b], zr_recv.at[xt, q],
                    {"fs": at(zs, y)})

    def fr_copy(b, i, zt):
        xt, ct, q = place(b)
        return send(part.at[b], fr.at[q, i], fr_send.at[b], fr_recv.at[q, i],
                    {"fs": at(zt, y), "tp": 2 * xt + ct})

    def roles(b):
        xt, ct, q = place(b)
        by_x, mine = first_x(ct, q), xt == x
        by_z = jnp.logical_not(by_x)
        other = xt != x
        return {
            "x": (by_x & other, xr_copy(b)),
            "z": (by_z & away, zr_copy(b)),
            "collect_x": (by_x & mine, None),
            "collect_z": (by_z & home, None),
            "final_z": (by_x & mine & away, fr_copy(b, 1, zs)),
            "final_x": (by_z & home & other, fr_copy(b, turn(xt), z)),
            "final_core": (mine & home & (ct != c), fr_copy(b, 0, z)),
            "final_own": (mine & home & (ct == c), None),
        }

    def block_at(k):
        return at(line_at(lax.rem(k, zz)), lax.rem(y + k // zz, yy))

    def down_block(k, s):
        b = block_at(k)

        @pl.when(jnp.logical_and(k >= 1, k + 1 < zz))
        def _():
            feed_relay(DOWN, k + 1)

        @pl.when(k + 1 >= zz)
        def _():
            @pl.when(k + 1 < n)
            def _():
                feed_share(DOWN, lax.rem(k + 1, zz), (k + 1) // zz)

        @pl.when(jnp.logical_or(b != f, away))
        def _():
            d_arrive(DOWN, b)

        part[b] = jnp.dot(hidden[...], full_down[b], preferred_element_type=F32).astype(BF16)
        way = roles(b)
        for key in ("x", "z"):
            wanted, copy = way[key]
            pl.when(wanted)(copy.start)
        return s

    lax.fori_loop(0, n, down_block, 0)

    def collect(k, s):
        b = block_at(k)
        xt, ct, q = place(b)
        way = roles(b)

        @pl.when(way["collect_x"][0])
        def _():
            for o in range(1, nx):
                got = xr.at[o - 1, ct, q]
                send(got, got, xr_send.at[b], xr_recv.at[o - 1, ct, q], {"tp": mate}).wait_recv()
            add_into(b, [xr.at[o - 1, ct, q] for o in range(1, nx)])

        @pl.when(way["collect_z"][0])
        def _():
            got = zr.at[xt, q]
            send(got, got, zr_send.at[b], zr_recv.at[xt, q], {"tp": mate}).wait_recv()
            add_into(b, [zr.at[xt, q]])

        for key in ("final_z", "final_x", "final_core"):
            wanted, copy = way[key]
            pl.when(wanted)(copy.start)

        @pl.when(way["final_own"][0])
        def _():
            fr[q, 0] = part[b]
        return s

    lax.fori_loop(0, n, collect, 0)

    def share_wait(q, i):
        got = fr.at[q, i]
        send(got, got, fr_send.at[0], fr_recv.at[q, i], {"tp": mate}).wait_recv()

    def final_sum(q, count):
        pl.when(away)(lambda: share_wait(q, 0))
        for i in range(1, count):
            share_wait(q, i)

        def body(i, s):
            rows = rows_of(i)
            total = fr[q, 0, rows, :].astype(F32)
            for j in range(1, count):
                total += fr[q, j, rows, :].astype(F32)
            total = total.astype(BF16)
            msum[rows, pl.ds(q * cols, cols)] = total
            if q:
                sq_own[1, :, rows] += squares_of(total)
            else:
                sq_own[1, :, rows] = squares_of(total)
            return s

        lax.fori_loop(0, tiles, body, 0)

    for q in range(bps):
        if nx == 2:
            final_sum(q, 2)
        else:
            pl.when(first_x(c, q))(lambda: final_sum(q, 2))
            pl.when(jnp.logical_not(first_x(c, q)))(lambda: final_sum(q, nx))

    square_open(1)

    def sent(b, s):
        way = roles(b)
        for key in ("x", "z", "final_z", "final_x", "final_core"):
            wanted, copy = way[key]
            pl.when(wanted)(copy.wait_send)
        return s

    lax.fori_loop(0, n, sent, 0)
    lax.fori_loop(0, tiles, first_done, 0)
    feed_close()
    square_close(1)

    def last_tile(i, c):
        rows = rows_of(i)
        level = level_of(1, rows)
        v = first[rows, :].astype(F32) + msum[rows, :].astype(F32) * level * output_gain[t]
        out[rows, :] = v.astype(BF16)
        return c

    lax.fori_loop(0, tiles, last_tile, 0)


def solution(mesh):
    n, nt = mesh.shape["fs"], mesh.shape["tp"]

    def shards(
        tokens, mixer_gain, conv_taps, outer_weight, inner_weight, value_weight, merge_weight,
        merge_gain, channel_gain, gate_weight, up_weight, down_weight, output_gain,
    ):
        length, width = tokens.shape
        blk, channels = outer_weight.shape
        units = gate_weight.shape[1]
        cols = merge_weight.shape[1]
        depth = width * nt
        bps = n // nt
        nx = nt // 2
        yy = plane_rows(n)
        zz = n // yy
        tiles = length // min(256, length)
        most = max(2, nx)

        def slabs(gain):
            return gain.reshape(nt, 1, width)

        vmem = pl.BlockSpec(memory_space=pltpu.VMEM)
        held = pl.BlockSpec(memory_space=pl.ANY)
        dma = pltpu.SemaphoreType.DMA
        return pl.pallas_call(
            lambda *refs: layer_kernel(n, nt, *refs),
            out_shape=jax.ShapeDtypeStruct((length, width), BF16),
            in_specs=[vmem] * 3 + [held] * 4 + [vmem] * 2 + [held] * 3 + [vmem],
            out_specs=vmem,
            scratch_shapes=[
                pltpu.VMEM((nt, length, width), BF16),
                pltpu.VMEM((length, depth), BF16),
                pltpu.VMEM((n * blk, channels), BF16),
                pltpu.VMEM((n * blk, channels), BF16),
                pltpu.VMEM((n * blk, channels), BF16),
                pltpu.VMEM((n, channels, cols), BF16),
                pltpu.VMEM((n * blk, units), BF16),
                pltpu.VMEM((n * blk, units), BF16),
                pltpu.VMEM((n, units, cols), BF16),
                pltpu.VMEM((length, channels), F32),
                pltpu.VMEM((length + 8, channels), F32),
                pltpu.VMEM((length, channels), BF16),
                pltpu.VMEM((n, length, cols), BF16),
                pltpu.VMEM((nx, bps, length, cols), BF16),
                pltpu.VMEM((nx - 1, bps, length, cols), BF16),
                pltpu.VMEM((length, width), BF16),
                pltpu.VMEM((length, width), BF16),
                pltpu.VMEM((nt, length, width), BF16),
                pltpu.VMEM((length, units), BF16),
                pltpu.VMEM((nx - 1, 2, bps, length, cols), BF16),
                pltpu.VMEM((nx, bps, length, cols), BF16),
                pltpu.VMEM((bps, most, length, cols), BF16),
                pltpu.VMEM((2, 8, length), F32),
                pltpu.VMEM((2, nt - 1, 8, length), F32),
                dma((2, 2, 4)),
                dma((2, 2, 4, n // 2)),
                dma((nt - 1,)), dma((nt - 1,)),
                dma((nx, bps)), dma((nx, bps)),
                dma((nx - 1, bps)), dma((nx - 1, bps)),
                dma((3, zz // 2, 2)), dma((3, zz)),
                dma((3, zz, yy - 1)), dma((3, n)),
                dma((3, n)), dma((3, n)),
                dma((nx + 1, tiles)), dma((nt, tiles)), dma((2, nx - 1, tiles)),
                dma((n,)), dma((nx - 1, 2, bps)),
                dma((n,)), dma((nx, bps)),
                dma((n,)), dma((bps, most)),
                dma((2, nt - 1)), dma((2, nt - 1)), dma((7,)),
            ],
            compiler_params=pltpu.CompilerParams(
                collective_id=0, has_side_effects=True, vmem_limit_bytes=67043328
            ),
        )(
            tokens, slabs(mixer_gain), conv_taps, outer_weight, inner_weight, value_weight,
            merge_weight, slabs(merge_gain), slabs(channel_gain), gate_weight, up_weight,
            down_weight, slabs(output_gain),
        )

    return jax.shard_map(
        shards,
        mesh=mesh,
        in_specs=(
            P("fs", "tp"), P(), P(), P("fs", "tp"), P("fs", "tp"), P("fs", "tp"), P("tp", "fs"),
            P(), P(), P("fs", "tp"), P("fs", "tp"), P("tp", "fs"), P(),
        ),
        out_specs=P("fs", "tp"),
        check_vma=False,
    )
```
